32 devices in a mesh: st: 16 (over z, y, x), tp: 2 (over core).
Axes of the slice: x: 2, y: 2, z: 4, core: 2. Of those that a mesh axis runs over, the one named last changes fastest.
Arguments:
- hidden: bfloat16 [16384, 2048], P('st'), may hold values from -6 to 6
- norm_gain: float32 [2048], replicated, may hold values from 0.1 to 1.9
- store: bfloat16 [384, 64, 2048], P('st'), may hold values from -6 to 6
- store_gain: float32 [2048], replicated, may hold values from 0.1 to 1.9
- passage_ids: int32 [128, 4], P('st'), may hold values from 0 to 383, as said below
- w_pool: bfloat16 [2048, 1024], P(None, 'tp'), may hold values from -0.125 to 0.125
- pool_mix: bfloat16 [4, 256, 256], P('tp'), may hold values from -0.375 to 0.375
- w_branch: bfloat16 [1024, 2048], P('tp'), may hold values from -0.1875 to 0.1875
- w_query: bfloat16 [2048, 512], P(None, 'tp'), may hold values from -0.125 to 0.125
- w_key: bfloat16 [2048, 512], P(None, 'tp'), may hold values from -0.125 to 0.125
- w_value: bfloat16 [2048, 512], P(None, 'tp'), may hold values from -0.125 to 0.125
- sharpness: float32 [4], P('tp'), may hold values from 1 to 90
- w_out: bfloat16 [512, 2048], P('tp'), may hold values from -0.25 to 0.25
- w_gate: bfloat16 [2048, 2048], P(None, 'tp'), may hold values from -0.125 to 0.125
Outputs:
- mixed: bfloat16 [16384, 2048], P('st', 'tp')
The draws below stay inside these ranges and needn't reach their ends.
Inputs may be any that keep to these rules, and one draw needn't show every extreme that they name: `passage_ids`: passage p lies on index p // 24 of st. The ids of one sequence's blocks (aligned rows of 32 ids) name passages of at most 4 reads on any one holder, counted with repeats, and some sequence reaches 4 at some holder in every draw.
All inputs are finite; a program needn't handle non-finite values.
Results may differ from the reference program's by a relative error of at most 0.0095.
The reference program's roundings to bfloat16 on the way (of `normed`, `pool_in`, `pooled`, `pool_out`, `query`, `passage_normed`, `weights` and `read`) count: a program that leaves them out, or rounds other values in their place, can miss the bound.
Values may be sent and summed in bfloat16 or wider, within the bound.
A program may use at most 128 MiB of HBM per device.

```python
import jax
import jax.numpy as jnp
from jax import lax

D = 2048
GROUPS = 4
GROUP_DIM = 256
XHEADS = 4
HEAD_DIM = 128
BLOCK = 128
PER_BLOCK = 4
PLEN = 64
PASS_DEV = 24
TOK_DEV = 1024
POOL_WIDTH = 1024
XWIDTH = 512
TOKENS = 16384
BLOCKS = 128
REQ_DEV = 32
MOST = 4
PASSAGES = 384
N_ST = 16
N_TP = 2


def draw_passage_ids(key, part):
    keys = jax.random.split(jax.random.fold_in(key, 11), 5)
    slots = N_ST * MOST
    devices = jnp.arange(N_ST)[:, None]
    slot_owner = jnp.broadcast_to(jnp.arange(slots)[None, :] // MOST, (N_ST, slots))
    forced = (slot_owner == (devices - 1) % N_ST) | (slot_owner == (devices + N_ST // 2) % N_ST)
    noise = jax.random.randint(keys[0], (N_ST, slots), 0, 1 << 20)
    score = jnp.where(forced, 0, noise + 1) * slots + jnp.arange(slots)[None, :]
    order = jnp.argsort(score, axis=1)[:, :REQ_DEV]
    chosen = jnp.take_along_axis(slot_owner, order, axis=1)
    shuffle = jax.random.randint(keys[1], (N_ST, REQ_DEV), 0, 1 << 20) * REQ_DEV + jnp.arange(REQ_DEV)[None, :]
    owners = jnp.take_along_axis(chosen, jnp.argsort(shuffle, axis=1), axis=1)
    local = jnp.minimum(jax.random.randint(keys[2], (N_ST, REQ_DEV), 0, PASS_DEV), jax.random.randint(keys[3], (N_ST, REQ_DEV), 0, PASS_DEV))
    local = jnp.minimum(local, jax.random.randint(keys[4], (N_ST, REQ_DEV), 0, PASS_DEV))
    return (owners * PASS_DEV + local).reshape(BLOCKS, PER_BLOCK).astype(jnp.int32)


def draw_sharpness(key, part):
    spread = jax.random.uniform(jax.random.fold_in(key, 23), (XHEADS,), jnp.float32)
    return jnp.exp(jnp.log(1.0) + spread * (jnp.log(4.0) - jnp.log(1.0)))


def steps_of(key, extent, cuts, low, largest):
    level, own = 1.0, jax.random.fold_in(key, 6)
    for dim, blocks in cuts:
        draws = jnp.exp(jax.random.uniform(jax.random.fold_in(own, dim), (blocks,), jnp.float32, low / len(cuts), largest / len(cuts)))
        level = level * jnp.repeat(draws, extent[dim] // blocks).reshape([-1 if axis == dim else 1 for axis in range(len(extent))])
    return level


def scatter_about(rng, extent, scale, reach, cuts=(), held_as=jnp.bfloat16):
    drawn = scale * jax.random.normal(rng, extent, jnp.float32)
    if cuts:
        drawn = drawn * steps_of(rng, extent, cuts, -0.22, 0.18)
    return jnp.clip(drawn, -reach, reach).astype(held_as)


def setup_inputs(seed: int = 0) -> dict:
    streams_of = jax.random.split(jax.random.key(seed), 15)
    hidden = scatter_about(streams_of[0], (TOKENS, D), 1.0, 6.0, ((0, 16),))
    norm_gain = jnp.clip(1.0 + 0.18 * jax.random.normal(streams_of[1], (D,), jnp.float32), 0.1, 1.9)
    store = scatter_about(streams_of[2], (PASSAGES, PLEN, D), 1.0, 6.0, ((0, 16),))
    store_gain = jnp.clip(1.0 + 0.18 * jax.random.normal(streams_of[3], (D,), jnp.float32), 0.1, 1.9)
    passage_ids = draw_passage_ids(jax.random.fold_in(streams_of[14], 71), 0)
    w_pool = scatter_about(streams_of[5], (D, POOL_WIDTH), D ** -0.5, 0.125, ((1, 2),))
    pool_mix = scatter_about(streams_of[6], (GROUPS, GROUP_DIM, GROUP_DIM), GROUP_DIM ** -0.5, 0.375, ((0, 2),))
    w_branch = scatter_about(streams_of[7], (POOL_WIDTH, D), POOL_WIDTH ** -0.5, 0.1875, ((0, 2),))
    w_query = scatter_about(streams_of[8], (D, XWIDTH), D ** -0.5, 0.125, ((1, 2),))
    w_key = scatter_about(streams_of[9], (D, XWIDTH), D ** -0.5, 0.125, ((1, 2),))
    w_value = scatter_about(streams_of[10], (D, XWIDTH), D ** -0.5, 0.125, ((1, 2),))
    sharpness = draw_sharpness(jax.random.fold_in(streams_of[14], 71), 0)
    w_out = scatter_about(streams_of[12], (XWIDTH, D), XWIDTH ** -0.5, 0.25, ((0, 2),))
    w_gate = scatter_about(streams_of[13], (D, D), D ** -0.5, 0.125, ((1, 2),))
    return {"hidden": hidden, "norm_gain": norm_gain, "store": store, "store_gain": store_gain, "passage_ids": passage_ids, "w_pool": w_pool, "pool_mix": pool_mix, "w_branch": w_branch, "w_query": w_query, "w_key": w_key, "w_value": w_value, "sharpness": sharpness, "w_out": w_out, "w_gate": w_gate}


def rms_norm(values, gain):
    wide = values.astype(jnp.float32)
    scale = lax.rsqrt(lax.optimization_barrier(jnp.mean(wide * wide, axis=-1, keepdims=True)) + 1e-05)
    return wide * scale * gain

def split_sum(left, right, pieces):
    width = left.shape[1] // pieces
    total = jnp.zeros((left.shape[0], right.shape[1]), jnp.float32)
    for index in range(pieces):
        term = jnp.dot(left[:, index * width:(index + 1) * width], right[index * width:(index + 1) * width], preferred_element_type=jnp.float32).astype(jnp.bfloat16)
        term = lax.optimization_barrier(term)
        total = total + term.astype(jnp.float32)
    return total

def reference(hidden, norm_gain, store, store_gain, passage_ids, w_pool, pool_mix, w_branch, w_query, w_key, w_value, sharpness, w_out, w_gate):
    normed = rms_norm(hidden, norm_gain).astype(jnp.bfloat16)
    pool_in = jnp.dot(normed, w_pool, preferred_element_type=jnp.float32).astype(jnp.bfloat16)
    grouped = pool_in.astype(jnp.float32).reshape(N_ST, TOK_DEV, GROUPS, GROUP_DIM)
    position = jnp.arange(TOK_DEV)
    outputs = []
    for group in range(GROUPS):
        window = 2 ** (group + 1)
        column = grouped[:, :, group]
        total = jnp.zeros_like(column)
        for shift in range(window):
            total = total + jnp.pad(column, ((0, 0), (shift, 0), (0, 0)))[:, :TOK_DEV]
        count = jnp.minimum(position + 1, window).astype(jnp.float32)[None, :, None]
        outputs.append(total / count - column)
    pooled = jnp.stack(outputs, axis=2).astype(jnp.bfloat16)
    pool_out = jnp.einsum('ntgc,gcd->ntgd', pooled.astype(jnp.float32), pool_mix.astype(jnp.float32))
    pool_out = pool_out.astype(jnp.bfloat16).reshape(TOKENS, POOL_WIDTH)
    branch_pool = split_sum(pool_out, w_branch, N_TP)
    query = jnp.dot(normed, w_query, preferred_element_type=jnp.float32).astype(jnp.bfloat16)
    query_blocks = query.reshape(BLOCKS, BLOCK, XHEADS, HEAD_DIM)
    scale = sharpness / HEAD_DIM ** 0.5

    def one_block(items):
        block_query, ids = items
        rows = store[ids].reshape(PER_BLOCK * PLEN, D)
        passage_normed = rms_norm(rows, store_gain).astype(jnp.bfloat16)
        keys = jnp.dot(passage_normed, w_key, preferred_element_type=jnp.float32).astype(jnp.bfloat16)
        values = jnp.dot(passage_normed, w_value, preferred_element_type=jnp.float32).astype(jnp.bfloat16)
        keys = keys.reshape(PER_BLOCK * PLEN, XHEADS, HEAD_DIM).astype(jnp.float32)
        values = values.reshape(PER_BLOCK * PLEN, XHEADS, HEAD_DIM).astype(jnp.float32)
        scores = jnp.einsum('qhd,khd->hqk', block_query.astype(jnp.float32), keys) * scale[:, None, None]
        weights = jax.nn.softmax(scores, axis=-1).astype(jnp.bfloat16)
        read = jnp.einsum('hqk,khd->qhd', weights.astype(jnp.float32), values)
        return read.astype(jnp.bfloat16).reshape(BLOCK, XWIDTH)
    read = lax.map(one_block, (query_blocks, passage_ids)).reshape(TOKENS, XWIDTH)
    branch_read = split_sum(read, w_out, N_TP)
    gate = jax.nn.sigmoid(jnp.dot(normed, w_gate, preferred_element_type=jnp.float32))
    return (branch_pool + gate * branch_read).astype(jnp.bfloat16)
```

```python
import functools
import math

import jax
import jax.numpy as jnp
from jax import lax
from jax.experimental import pallas as pl
from jax.experimental.pallas import tpu as pltpu
from jax.sharding import PartitionSpec as P

MESH = pl.DeviceIdType.MESH
F32 = jnp.float32
BF16 = jnp.bfloat16
ANY = pl.BlockSpec(memory_space=pl.ANY)
VMEM = pl.BlockSpec(memory_space=pltpu.VMEM)
SMEM = pl.BlockSpec(memory_space=pltpu.SMEM)
LIMIT = 66_000_000


def planes_of(mesh):
    heights = {getattr(d, "coords", (0, 0, 0))[2] for d in mesh.devices.flat}
    return len(heights)


def rms_rows(wide, gain):
    scale = lax.rsqrt(jnp.mean(wide * wide, axis=-1, keepdims=True) + 1e-05)
    return wide * scale * gain


def project_kernel(
    holders, pieces, ids_ref, store_ref, gain_ref, wk_ref, wv_ref, all_ref, kv_ref, rows, load_sem, send_sem, recv_sem
):
    me = lax.axis_index("st")
    core = lax.axis_index("tp")
    piece = rows.shape[0] // pieces
    width = wk_ref.shape[1]
    length = kv_ref.shape[1]
    passages = piece // length

    def load(i):
        return pltpu.make_async_copy(
            store_ref.at[pl.ds(i * piece, piece)], rows.at[pl.ds(i * piece, piece)], load_sem.at[i]
        )

    for i in range(pieces):
        load(i).start()

    barrier = pltpu.get_barrier_semaphore()

    def other(step):
        return lax.rem(me + step, holders)

    def greet(step, carry):
        pl.semaphore_signal(barrier, inc=1, device_id=(other(step), core), device_id_type=MESH)
        return carry

    lax.fori_loop(1, holders, greet, 0)
    pl.semaphore_wait(barrier, holders - 1)

    def ids_copy(step):
        return pltpu.make_async_remote_copy(
            src_ref=ids_ref,
            dst_ref=all_ref.at[me],
            send_sem=send_sem.at[step],
            recv_sem=recv_sem.at[step],
            device_id=(other(step), core),
            device_id_type=MESH,
        )

    def send(step, carry):
        ids_copy(step).start()
        return carry

    lax.fori_loop(1, holders, send, 0)
    all_ref[me] = ids_ref[...]

    def project(i, carry):
        load(i).wait()
        start = pl.multiple_of(i * piece, piece)
        normed = rms_rows(rows[pl.ds(start, piece), :].astype(F32), gain_ref[...]).astype(BF16)
        for half, w_ref in enumerate((wk_ref, wv_ref)):
            part = jnp.dot(normed, w_ref[...], preferred_element_type=F32).astype(BF16)
            kv_ref[pl.ds(i * passages, passages), :, half * width : (half + 1) * width] = part.reshape(
                passages, length, width
            )
        return carry

    lax.fori_loop(0, pieces, project, 0)

    def finish(step, carry):
        ids_copy(step).wait()
        return carry

    lax.fori_loop(1, holders, finish, 0)


def project(ids, store, store_gain, w_key, w_value):
    holders = lax.axis_size("st")
    pass_dev, length, model = store.shape
    pieces = math.gcd(pass_dev, 6)
    width = w_key.shape[1]
    reads = ids.shape[0]
    padded = jnp.pad(ids.reshape(1, reads), ((0, 7), (0, 128 - reads)))
    return pl.pallas_call(
        functools.partial(project_kernel, holders, pieces),
        out_shape=(
            jax.ShapeDtypeStruct((holders, 8, 128), jnp.int32),
            jax.ShapeDtypeStruct((pass_dev, length, 2 * width), BF16),
        ),
        in_specs=[VMEM, ANY, VMEM, VMEM, VMEM],
        out_specs=(VMEM, VMEM),
        scratch_shapes=[
            pltpu.VMEM((pass_dev * length, model), BF16),
            pltpu.SemaphoreType.DMA((pieces,)),
            pltpu.SemaphoreType.DMA((holders,)),
            pltpu.SemaphoreType.DMA((holders,)),
        ],
        compiler_params=pltpu.CompilerParams(collective_id=0, has_side_effects=True, vmem_limit_bytes=LIMIT),
        cost_estimate=pl.CostEstimate(
            flops=4 * pass_dev * length * model * width, bytes_accessed=store.size * 2, transcendentals=0
        ),
    )(padded, store.reshape(pass_dev * length, model), store_gain.reshape(1, model), w_key, w_value)


def plan(ids, planes, pass_dev, most, caps):
    holders, reads = ids.shape
    side = holders // planes
    me = lax.axis_index("st")
    z, c = lax.div(me, side), lax.rem(me, side)
    i32 = jnp.int32
    everything = jnp.arange(holders * pass_dev, dtype=i32)
    need = jnp.any(ids.reshape(planes, side * reads, 1) == everything, axis=1)
    need = need.reshape(planes, planes, side, pass_dev)
    at = jnp.arange(planes, dtype=i32)
    ahead = (at[:, None] - at[None, :])[:, :, None, None]
    far = [jnp.max(jnp.where(need, jnp.maximum(sign * ahead, 0), 0), axis=0) for sign in (1, -1)]
    fits = []
    for way, reach in enumerate(far):
        for d in range(1, planes):
            count = jnp.sum((reach >= d).astype(i32), axis=2)
            left = [(planes - q - d) if way == 0 else (q - d + 1) for q in range(planes)]
            room = jnp.array([caps[k - 1] if k >= 1 else pass_dev for k in left], i32)
            fits.append(jnp.all(count <= room[:, None]))
    fits = jnp.all(jnp.stack(fits))

    lane = jnp.arange(pass_dev, dtype=i32)
    column = jnp.stack([lax.dynamic_index_in_dim(reach, c, axis=1, keepdims=False) for reach in far])
    before = (column[:, :, None, :] > column[:, :, :, None]) | (
        (column[:, :, None, :] == column[:, :, :, None]) & (lane[None, :] < lane[:, None])
    )
    place = jnp.sum(before.astype(i32), axis=3)
    own = lax.dynamic_index_in_dim(place, z, axis=1, keepdims=False)
    order = jnp.sum(jnp.where(own[:, None, :] == lane[None, :, None], lane, 0), axis=2)

    q = at[:, None]
    where_at = jnp.where(q == z, lane[None, :], jnp.where(q < z, place[0], place[1]))
    mine = lax.dynamic_slice_in_dim(ids, z * side, side, axis=0)
    holder = lax.div(mine, pass_dev)
    inside = mine - holder * pass_dev
    step = jnp.arange(reads, dtype=i32)
    earlier = (holder[:, None, :] == holder[:, :, None]) & (step[None, :] < step[:, None])
    rank = jnp.sum(earlier.astype(i32), axis=2)
    hq, hc = lax.div(holder, side), lax.rem(holder, side)
    flat = jnp.where(hc == c, hq * pass_dev + inside, -1)
    found = jnp.sum(
        jnp.where(
            flat[:, :, None] == jnp.arange(planes * pass_dev, dtype=i32), where_at.reshape(-1), 0
        ),
        axis=2,
    )
    target = jnp.where(hc == c, hq * most + rank, -1)
    pick = jnp.sum(
        jnp.where(target[:, None, :] == jnp.arange(planes * most, dtype=i32)[None, :, None], found[:, None, :], 0),
        axis=2,
    )
    slots = (hc * planes + hq) * most + rank
    slots = lax.dynamic_index_in_dim(slots, c, axis=0, keepdims=False)
    return fits, jnp.concatenate([order.reshape(-1), pick.reshape(-1), slots])


def chunks_of(caps):
    cut = [(0, caps[0] // 2, 1), (caps[0] // 2, caps[0], 1)]
    for k in range(1, len(caps)):
        if caps[k] > caps[k - 1]:
            cut.append((caps[k - 1], caps[k], k + 1))
    return cut


def mixer_kernel(
    planes,
    caps,
    most,
    block_len,
    tab,
    scale_ref,
    gain_ref,
    mix_ref,
    kv_hbm,
    hidden_hbm,
    w_pool_hbm,
    w_query_hbm,
    w_gate_hbm,
    w_branch_hbm,
    w_out_hbm,
    out_ref,
    kv,
    normed,
    w_pool,
    w_query,
    w_gate,
    w_branch,
    w_branch_far,
    w_out,
    w_out_far,
    pool_in,
    pool_out,
    pool_far,
    branch,
    gate,
    query,
    read,
    read_far,
    own_lists,
    *rest,
):
    reach = planes - 1
    lists = [rest[w * reach : (w + 1) * reach] for w in range(2)]
    picked, final, load_sem, z_send, z_recv, in_send, in_recv, core_send, core_recv = rest[2 * reach :]
    holders = lax.axis_size("st")
    side = holders // planes
    me = lax.axis_index("st")
    core = lax.axis_index("tp")
    z, c = lax.div(me, side), lax.rem(me, side)
    tokens, model = normed.shape
    half = out_ref.shape[1]
    pass_dev = kv.shape[0]
    cuts = chunks_of(caps)
    beyond = (planes - 1 - z, z)
    behind = (z, planes - 1 - z)
    step_to = (side, -side)

    mine = pl.ds(pl.multiple_of(core * half, half), half)
    theirs = pl.ds(pl.multiple_of((1 - core) * half, half), half)
    loads = [
        pltpu.make_async_copy(src, dst, load_sem.at[i])
        for i, (src, dst) in enumerate(
            (
                (kv_hbm, kv),
                (hidden_hbm, normed),
                (w_pool_hbm, w_pool),
                (w_query_hbm, w_query),
                (w_branch_hbm.at[:, mine], w_branch),
                (w_gate_hbm, w_gate),
                (w_out_hbm.at[:, mine], w_out),
            )
        )
    ]
    for copy in loads:
        copy.start()

    barrier = pltpu.get_barrier_semaphore()

    def greet(device):
        pl.semaphore_signal(barrier, inc=1, device_id=device, device_id_type=MESH)

    plane_mates = [z * side + lax.rem(c + rel, side) for rel in range(1, side)]
    for mate in plane_mates:
        greet((mate, core))
    greet((me, 1 - core))
    for way in range(2):
        pl.when(beyond[way] >= 1)(lambda way=way: greet((me + step_to[way], core)))
    pl.semaphore_wait(barrier, side + (z + reach - 1) // reach + (beyond[0] + reach - 1) // reach)

    def partner(src, dst, i):
        return pltpu.make_async_remote_copy(
            src_ref=src,
            dst_ref=dst,
            send_sem=core_send.at[i],
            recv_sem=core_recv.at[i],
            device_id=(me, 1 - core),
            device_id_type=MESH,
        )

    weight_swaps = [
        partner(w_branch_hbm.at[:, theirs], w_branch_far, 0),
        partner(w_out_hbm.at[:, theirs], w_out_far, 1),
    ]
    pool_swap = partner(pool_out, pool_far, 2)

    def hop(way, d, i):
        first, last, _ = cuts[i]
        src = own_lists.at[way] if d == 0 else lists[way][d - 1]
        return pltpu.make_async_remote_copy(
            src_ref=src.at[pl.ds(first, last - first)],
            dst_ref=lists[way][d].at[pl.ds(first, last - first)],
            send_sem=z_send.at[way, d, i],
            recv_sem=z_recv.at[way, d, i],
            device_id=(me + step_to[way], core),
            device_id_type=MESH,
        )

    def arrive(way, d, i):
        first, last, _ = cuts[i]
        ref = lists[way][d - 1].at[pl.ds(first, last - first)]
        pltpu.make_async_remote_copy(
            src_ref=ref,
            dst_ref=ref,
            send_sem=z_send.at[way, d - 1, i],
            recv_sem=z_recv.at[way, d - 1, i],
            device_id=(me, 1 - core),
            device_id_type=MESH,
        ).wait_recv()

    def forward(d, i):
        need = cuts[i][2]
        if need > reach - d:
            return
        for way in range(2):

            def go(way=way):
                arrive(way, d, i)
                hop(way, d, i).start()

            pl.when((behind[way] >= d) & (beyond[way] >= need))(go)

    def keep(d):
        for i, (_, _, need) in enumerate(cuts):
            if need > reach - d + 1:
                continue
            for way in range(2):
                pl.when((behind[way] >= d) & (beyond[way] + 1 == need))(lambda way=way, i=i: arrive(way, d, i))

    base = 2 * pass_dev

    def spread_copy(rel, q):
        mate = z * side + lax.rem(c + rel, side)
        return pltpu.make_async_remote_copy(
            src_ref=picked.at[rel - 1, pl.ds(q * most, most)],
            dst_ref=final.at[pl.ds((c * planes + q) * most, most)],
            send_sem=in_send.at[rel - 1, q],
            recv_sem=in_recv.at[c * planes + q],
            device_id=(mate, core),
            device_id_type=MESH,
        )

    def spread(src, q):
        for rel in range(1, side):
            mate = lax.rem(c + rel, side)
            for j in range(most):
                picked[rel - 1, q * most + j] = src[tab[base + (mate * planes + q) * most + j]]
        for rel in range(1, side):
            spread_copy(rel, q).start()
        for j in range(most):
            final[(c * planes + q) * most + j] = src[tab[base + (c * planes + q) * most + j]]

    def spread_from(d):
        for way in range(2):
            q = z - d if way == 0 else z + d
            pl.when(behind[way] >= d)(lambda way=way, q=q: spread(lists[way][d - 1], q))

    loads[0].wait()
    for way in range(2):
        for s in range(caps[-1]):
            own_lists[way, s] = kv[tab[way * pass_dev + s]]
    for i, (_, _, need) in enumerate(cuts):
        for way in range(2):
            pl.when(beyond[way] >= need)(lambda way=way, i=i: hop(way, 0, i).start())
    spread(kv, z)
    for copy in weight_swaps:
        copy.start()

    def norm(lo, hi, rows=32):
        def body(i, carry):
            at = pl.ds(pl.multiple_of(i * rows, rows), rows)
            normed[at, :] = rms_rows(normed[at, :].astype(F32), gain_ref[...]).astype(BF16)
            return carry

        lax.fori_loop(lo // rows, hi // rows, body, 0)

    piece = math.gcd(tokens, 256)
    pieces = tokens // piece
    halo = pool_in.shape[0] - tokens
    groups, group_dim = mix_ref.shape[:2]

    def project_rows(lo, hi):
        def body(i, carry):
            at = pl.ds(pl.multiple_of(i * piece, piece), piece)
            rows = normed[at, :]
            pool_in[pl.ds(pl.multiple_of(halo + i * piece, halo), piece), :] = jnp.dot(
                rows, w_pool[...], preferred_element_type=F32
            ).astype(BF16)
            query[at, :] = jnp.dot(rows, w_query[...], preferred_element_type=F32).astype(BF16)
            return carry

        lax.fori_loop(lo, hi, body, 0)

    def pool_rows(i, carry):
        at = pl.ds(pl.multiple_of(i * piece, piece), piece)
        position = i * piece + lax.broadcasted_iota(jnp.int32, (piece, 1), 0)
        for g in range(groups):
            cols = slice(g * group_dim, (g + 1) * group_dim)
            wide = pool_in[pl.ds(pl.multiple_of(i * piece, piece), piece + halo), cols].astype(F32)
            sums = []
            total = wide
            shift = 1
            while shift < halo:
                total = total + pltpu.roll(total, shift, 0)
                sums.append(total[halo:])
                shift *= 2
            per_core = [sums[k * groups + g] for k in range(len(sums) // groups)]
            level = per_core[0]
            window = 2 ** (g + 1)
            for k in range(1, len(per_core)):
                level = jnp.where(core == k, per_core[k], level)
                window = jnp.where(core == k, 2 ** (k * groups + g + 1), window)
            count = jnp.minimum(position + 1, window).astype(F32)
            pooled = (level / count - wide[halo:]).astype(BF16)
            pool_out[at, cols] = jnp.dot(pooled, mix_ref[g], preferred_element_type=F32).astype(BF16)
        return carry

    def gate_rows(lo, hi):
        def body(i, carry):
            at = pl.ds(pl.multiple_of(i * piece, piece), piece)
            for j in range(2):
                cols = slice(j * half // 2, (j + 1) * half // 2)
                logits = jnp.dot(normed[at, :], w_gate[:, cols], preferred_element_type=F32)
                gate[at, cols] = 1.0 / (1.0 + jnp.exp(-logits))
            return carry

        lax.fori_loop(lo, hi, body, 0)

    def two_terms(a, w, a_far, w_far):
        near = jnp.dot(a, w, preferred_element_type=F32).astype(BF16).astype(F32)
        far = jnp.dot(a_far, w_far, preferred_element_type=F32).astype(BF16).astype(F32)
        return near + far

    def branch_rows(i, carry):
        at = pl.ds(pl.multiple_of(i * piece, piece), piece)
        for j in range(2):
            cols = slice(j * half // 2, (j + 1) * half // 2)
            branch[at, cols] = two_terms(
                pool_out[at, :], w_branch[:, cols], pool_far[at, :], w_branch_far[:, cols]
            )
        return carry

    def forward_all(d, which):
        for i in which:
            if i < len(cuts):
                forward(d, i)

    loads[1].wait()
    norm(0, tokens)
    loads[2].wait()
    loads[3].wait()
    pool_in[:halo, :] = jnp.zeros((halo, pool_in.shape[1]), BF16)
    project_rows(0, pieces)
    forward_all(1, [0])
    lax.fori_loop(0, pieces, pool_rows, 0)
    pool_swap.start()
    loads[5].wait()
    gate_rows(0, pieces // 2)
    forward_all(1, [1])
    gate_rows(pieces // 2, pieces)
    loads[4].wait()
    loads[6].wait()
    for copy in weight_swaps:
        copy.wait()
    pool_swap.wait()
    lax.fori_loop(0, pieces, branch_rows, 0)
    forward_all(1, range(2, len(cuts)))
    keep(1)
    spread_from(1)
    for d in range(2, planes):
        if d < planes - 1:
            forward_all(d, range(len(cuts)))
        keep(d)
        spread_from(d)

    for rel in range(1, side):
        source = lax.rem(c + side - rel, side)
        for q in range(planes):
            at = pl.ds((source * planes + q) * most, most)
            pltpu.make_async_remote_copy(
                src_ref=final.at[at],
                dst_ref=final.at[at],
                send_sem=in_send.at[rel - 1, q],
                recv_sem=in_recv.at[source * planes + q],
                device_id=(me, 1 - core),
                device_id_type=MESH,
            ).wait_recv()

    blocks = tokens // block_len
    heads = scale_ref.shape[0]
    width = query.shape[1]
    head_dim = width // heads
    slot_base = base + side * planes * most
    per_block = (tab.shape[0] - slot_base) // blocks

    def read_swap(b):
        at = pl.ds(pl.multiple_of(b * block_len, block_len), block_len)
        return partner(read.at[at], read_far.at[at], 3 + b)

    def attend(b, carry):
        at = pl.ds(pl.multiple_of(b * block_len, block_len), block_len)
        memory = jnp.concatenate(
            [final[tab[slot_base + b * per_block + i]] for i in range(per_block)], axis=0
        )
        for h in range(heads):
            cut = slice(h * head_dim, (h + 1) * head_dim)
            scores = lax.dot_general(
                query[at, cut], memory[:, cut], (((1,), (1,)), ((), ())), preferred_element_type=F32
            )
            scores = scores * scale_ref[h]
            top = jnp.exp(scores - jnp.max(scores, axis=-1, keepdims=True))
            weights = (top * (1.0 / jnp.sum(top, axis=-1, keepdims=True))).astype(BF16)
            read[at, cut] = jnp.dot(
                weights, memory[:, width + h * head_dim : width + (h + 1) * head_dim], preferred_element_type=F32
            ).astype(BF16)
        read_swap(b).start()
        return carry

    lax.fori_loop(0, blocks, attend, 0)

    def finish(b, carry):
        at = pl.ds(pl.multiple_of(b * block_len, block_len), block_len)
        read_swap(b).wait()
        for j in range(2):
            cols = slice(j * half // 2, (j + 1) * half // 2)
            terms = two_terms(read[at, :], w_out[:, cols], read_far[at, :], w_out_far[:, cols])
            out_ref[at, cols] = (branch[at, cols] + gate[at, cols] * terms).astype(BF16)
        return carry

    lax.fori_loop(0, blocks, finish, 0)

    for way in range(2):
        for i, (_, _, need) in enumerate(cuts):
            for d in range(reach - need + 1):
                pl.when((behind[way] >= d) & (beyond[way] >= need))(
                    lambda way=way, d=d, i=i: hop(way, d, i).wait_send()
                )
    for rel in range(1, side):
        for q in range(planes):
            spread_copy(rel, q).wait_send()


def mixer(planes, caps, most, block_len, collective_id, operands):
    tab, scale, gain, mix, kv, hidden, w_pool, w_query, w_gate, w_branch, w_out = operands
    holders = lax.axis_size("st")
    side = holders // planes
    reach = planes - 1
    tokens, model = hidden.shape
    half = w_gate.shape[1]
    pool_width, width = w_pool.shape[1], w_query.shape[1]
    slot = kv.shape[1:]
    cores = lax.axis_size("tp")
    halo = 2 ** (cores * mix.shape[0])
    nch = len(chunks_of(caps))
    blocks = tokens // block_len
    v = pltpu.VMEM
    dma = pltpu.SemaphoreType.DMA
    flops = 2 * tokens * (model * (pool_width + width + half) + 2 * (pool_width + width) * half)
    return pl.pallas_call(
        functools.partial(mixer_kernel, planes, caps, most, block_len),
        out_shape=jax.ShapeDtypeStruct((tokens, half), BF16),
        in_specs=[SMEM, SMEM, VMEM, VMEM] + [ANY] * 7,
        out_specs=VMEM,
        scratch_shapes=[
            v(kv.shape, BF16),
            v(hidden.shape, BF16),
            v(w_pool.shape, BF16),
            v(w_query.shape, BF16),
            v(w_gate.shape, BF16),
            v((pool_width, half), BF16),
            v((pool_width, half), BF16),
            v((width, half), BF16),
            v((width, half), BF16),
            v((tokens + halo, pool_width), BF16),
            v((tokens, pool_width), BF16),
            v((tokens, pool_width), BF16),
            v((tokens, half), F32),
            v((tokens, half), F32),
            v((tokens, width), BF16),
            v((tokens, width), BF16),
            v((tokens, width), BF16),
            v((2, caps[-1], *slot), BF16),
            *[v((caps[reach - d], *slot), BF16) for _ in range(2) for d in range(1, planes)],
            v((side - 1, planes * most, *slot), BF16),
            v((holders * most, *slot), BF16),
            dma((7,)),
            dma((2, reach, nch)),
            dma((2, reach, nch)),
            dma((side - 1, planes)),
            dma((holders,)),
            dma((3 + blocks,)),
            dma((3 + blocks,)),
        ],
        compiler_params=pltpu.CompilerParams(
            collective_id=collective_id, has_side_effects=True, vmem_limit_bytes=LIMIT
        ),
        cost_estimate=pl.CostEstimate(flops=flops, bytes_accessed=32 * 2**20, transcendentals=0),
    )(*operands)


def body(
    planes,
    hidden,
    norm_gain,
    store,
    store_gain,
    passage_ids,
    w_pool,
    pool_mix,
    w_branch,
    w_query,
    w_key,
    w_value,
    sharpness,
    w_out,
    w_gate,
):
    holders = lax.axis_size("st")
    side = holders // planes
    blocks, per_block = passage_ids.shape
    reads = blocks * per_block
    pass_dev = store.shape[0]
    tokens, model = hidden.shape
    most = max(1, 2 * reads // holders)
    head_dim = w_query.shape[1] // sharpness.shape[0]

    all_ids, own_kv = project(passage_ids.reshape(-1), store, store_gain, w_key, w_value)
    one = min(pass_dev, side * most)
    full = tuple(min(pass_dev, k * one) for k in range(1, planes))
    short = tuple(min(f, (11 * one) // 16 + (k > 0) * pass_dev // 6 + (k > 1) * pass_dev // 12) for k, f in enumerate(full))
    fits, tab = plan(all_ids[:, 0, :reads], planes, pass_dev, most, short)
    operands = (
        tab,
        sharpness / math.sqrt(head_dim),
        norm_gain.reshape(1, model),
        pool_mix,
        own_kv,
        hidden,
        w_pool,
        w_query,
        w_gate,
        w_branch,
        w_out,
    )
    run = functools.partial(mixer, planes)
    block_len = tokens // blocks
    return lax.cond(
        fits,
        lambda *ops: run(short, most, block_len, 1, ops),
        lambda *ops: run(full, most, block_len, 2, ops),
        *operands,
    )


def solution(mesh):
    placed = (
        P("st", None),
        P(),
        P("st", None, None),
        P(),
        P("st", None),
        P(None, "tp"),
        P("tp", None, None),
        P("tp", None),
        P(None, "tp"),
        P(None, "tp"),
        P(None, "tp"),
        P("tp"),
        P("tp", None),
        P(None, "tp"),
    )
    return jax.shard_map(
        functools.partial(body, planes_of(mesh)), mesh=mesh, in_specs=placed, out_specs=P("st", "tp"), check_vma=False
    )
```

```python
import functools
import math

import jax
import jax.numpy as jnp
from jax import lax
from jax.experimental import pallas as pl
from jax.experimental.pallas import tpu as pltpu
from jax.sharding import PartitionSpec as P

MESH = pl.DeviceIdType.MESH
F32 = jnp.float32
BF16 = jnp.bfloat16
ANY = pl.BlockSpec(memory_space=pl.ANY)
VMEM = pl.BlockSpec(memory_space=pltpu.VMEM)
SMEM = pl.BlockSpec(memory_space=pltpu.SMEM)
LIMIT = 66_000_000


def planes_of(mesh):
    heights = {getattr(d, "coords", (0, 0, 0))[2] for d in mesh.devices.flat}
    return len(heights)


def rms_rows(wide, gain):
    scale = lax.rsqrt(jnp.mean(wide * wide, axis=-1, keepdims=True) + 1e-05)
    return wide * scale * gain


def plan_tables(holders, planes, reads, pass_dev, most, variants, all_ref, tab_ref):
    side = holders // planes
    lanes = 128
    per = lanes // reads
    me = lax.axis_index("st")
    z, c = lax.div(me, side), lax.rem(me, side)

    def lane_of(rows):
        return lax.broadcasted_iota(jnp.int32, (rows, lanes), 1).astype(F32)

    def sub_of(rows, width=lanes):
        return lax.broadcasted_iota(jnp.int32, (rows, width), 0).astype(F32)

    def whole(x, by):
        return jnp.floor((x + 0.5) * (1.0 / by))

    segment = whole(lane_of(1), reads)

    def requests(plane):
        return [requests_row(all_ref, plane, side, per, r, segment) for r in range(side // per)]

    holder_at = lax.broadcasted_iota(jnp.int32, (1, holders), 1).astype(F32)
    plane_at = whole(holder_at, side)
    far_up = jnp.zeros((pass_dev, holders), F32)
    far_down = jnp.zeros((pass_dev, holders), F32)
    for p in range(planes):
        hits = jnp.zeros((pass_dev, holders), F32)
        for row in requests(p):
            owner = whole(row, pass_dev)
            inside = row - owner * pass_dev
            a = jnp.where(inside == sub_of(pass_dev), 1.0, 0.0).astype(BF16)
            b = jnp.where(owner == sub_of(holders), 1.0, 0.0).astype(BF16)
            hits = hits + lax.dot_general(a, b, (((1,), (1,)), ((), ())), preferred_element_type=F32)
        ahead = jnp.where(hits > 0.5, p - plane_at, 0.0)
        far_up = jnp.maximum(far_up, ahead)
        far_down = jnp.maximum(far_down, -ahead)

    longest = [jnp.zeros((1, holders), F32) for _ in range(planes - 1)]
    for reach, left in ((far_up, planes - 1 - plane_at), (far_down, plane_at)):
        for d in range(1, planes):
            count = jnp.sum(jnp.where(reach >= d, 1.0, 0.0), axis=0, keepdims=True)
            for k in range(planes - 1):
                longest[k] = jnp.maximum(longest[k], jnp.where(left - d == k, count, 0.0))
    longest = [jnp.max(x, axis=1, keepdims=True) for x in longest]
    variant = jnp.zeros((1, 1), F32)
    for caps in variants[:-1]:
        over = jnp.zeros((1, 1), F32)
        for k, room in enumerate(caps):
            over = jnp.maximum(over, jnp.where(longest[k] > room, 1.0, 0.0))
        variant = variant + over

    lower = lax.broadcasted_iota(jnp.int32, (pass_dev, pass_dev), 1) < lax.broadcasted_iota(
        jnp.int32, (pass_dev, pass_dev), 0
    )
    diagonal = lax.broadcasted_iota(jnp.int32, (pass_dev, pass_dev), 1) == lax.broadcasted_iota(
        jnp.int32, (pass_dev, pass_dev), 0
    )

    def place_in(reach, q):
        col = jnp.sum(jnp.where(holder_at == (q * side + c).astype(F32), reach, 0.0), axis=1, keepdims=True)
        row = jnp.sum(jnp.where(diagonal, col, 0.0), axis=0, keepdims=True)
        before = (row > col) | ((row == col) & lower)
        return jnp.sum(jnp.where(before, 1.0, 0.0), axis=1, keepdims=True)

    number = sub_of(pass_dev)
    orders = [
        jnp.sum(jnp.where(place_in(reach, z) == lane_of(pass_dev), number, 0.0), axis=0, keepdims=True)
        for reach in (far_up, far_down)
    ]
    where_at = []
    for q in range(planes):
        place = place_in(jnp.where(q < z, far_up, far_down), jnp.int32(q))
        where_at.append(jnp.where(q == z, sub_of(pass_dev, 1), place))

    square_sub = sub_of(lanes)
    square_lane = lane_of(lanes)
    close = (square_sub < square_lane) & (whole(square_sub, reads) == whole(square_lane, reads))
    picks = jnp.zeros((planes * most, lanes), F32)
    slots = jnp.zeros((1, lanes), F32)
    for r, row in enumerate(requests(z)):
        owner = whole(row, pass_dev)
        inside = row - owner * pass_dev
        owner_col = jnp.sum(jnp.where(square_sub == square_lane, owner, 0.0), axis=1, keepdims=True)
        rank = jnp.sum(jnp.where(close & (owner_col == owner), 1.0, 0.0), axis=0, keepdims=True)
        of_plane = whole(owner, side)
        of_side = owner - of_plane * side
        here = of_side == c.astype(F32)
        found = jnp.zeros((1, lanes), F32)
        for q in range(planes):
            hit = here & (of_plane == q) & (inside == number)
            found = found + jnp.sum(jnp.where(hit, where_at[q], 0.0), axis=0, keepdims=True)
        target = jnp.where(here, of_plane * most + rank, -1.0)
        values = jnp.where(target == sub_of(planes * most), found, 0.0)
        for t in range(per):
            column = jnp.sum(jnp.where(segment == t, values, 0.0), axis=1, keepdims=True)
            picks = jnp.where(lane_of(planes * most) == r * per + t, column, picks)
        slots = jnp.where(lax.div(c, per) == r, (of_side * planes + of_plane) * most + rank, slots)
    for i, row in enumerate((*orders, slots, variant + jnp.zeros((1, lanes), F32))):
        tab_ref[i : i + 1, :] = row.astype(jnp.int32)
    tab_ref[8 : 8 + planes * most, :] = picks.astype(jnp.int32)


def requests_row(all_ref, plane, side, per, r, segment):
    row = jnp.zeros(segment.shape, F32)
    for t in range(per):
        ids = all_ref[plane * side + r * per + t][0:1, :].astype(F32)
        row = jnp.where(segment == t, ids, row)
    return row


def project_kernel(
    holders,
    planes,
    pieces,
    most,
    variants,
    ids_ref,
    store_ref,
    gain_ref,
    wk_ref,
    wv_ref,
    tab_ref,
    kv_ref,
    rows,
    mine_ids,
    all_ref,
    load_sem,
    send_sem,
    recv_sem,
):
    me = lax.axis_index("st")
    core = lax.axis_index("tp")
    piece = rows.shape[0] // pieces
    width = wk_ref.shape[1]
    pass_dev, length, _ = kv_ref.shape
    passages = piece // length
    blocks, per_block = ids_ref.shape
    reads = blocks * per_block

    def load(i):
        return pltpu.make_async_copy(
            store_ref.at[pl.ds(i * piece, piece)], rows.at[pl.ds(i * piece, piece)], load_sem.at[i]
        )

    for i in range(pieces):
        load(i).start()

    barrier = pltpu.get_barrier_semaphore()

    def other(step):
        return lax.rem(me + step, holders)

    def greet(step, carry):
        pl.semaphore_signal(barrier, inc=1, device_id=(other(step), core), device_id_type=MESH)
        return carry

    lax.fori_loop(1, holders, greet, 0)

    lane = lax.broadcasted_iota(jnp.int32, (blocks, 128), 1)
    lane = lane - reads * jnp.floor((lane.astype(F32) + 0.5) * (1.0 / reads)).astype(jnp.int32)
    block = jnp.floor((lane.astype(F32) + 0.5) * (1.0 / per_block)).astype(jnp.int32)
    inner = lane - block * per_block
    spread_ids = jnp.zeros((blocks, 128), F32)
    for k in range(per_block):
        spread_ids = jnp.where(inner == k, ids_ref[:, k : k + 1].astype(F32), spread_ids)
    at_block = lax.broadcasted_iota(jnp.int32, (blocks, 128), 0) == block
    row = jnp.sum(jnp.where(at_block, spread_ids, 0.0), axis=0, keepdims=True)
    mine_ids[...] = jnp.broadcast_to(row, mine_ids.shape).astype(jnp.int32)
    all_ref[me] = jnp.broadcast_to(row, mine_ids.shape).astype(jnp.int32)

    def project(i, carry):
        load(i).wait()
        start = pl.multiple_of(i * piece, piece)
        normed = rms_rows(rows[pl.ds(start, piece), :].astype(F32), gain_ref[...]).astype(BF16)
        for half, w_ref in enumerate((wk_ref, wv_ref)):
            part = jnp.dot(normed, w_ref[...], preferred_element_type=F32).astype(BF16)
            kv_ref[pl.ds(i * passages, passages), :, half * width : (half + 1) * width] = part.reshape(
                passages, length, width
            )
        return carry

    first = pieces // 2
    with jax.named_scope("kv0"):
        lax.fori_loop(0, first, project, 0)
    with jax.named_scope("greet_all"):
        pl.semaphore_wait(barrier, holders - 1)

    def ids_copy(step):
        return pltpu.make_async_remote_copy(
            src_ref=mine_ids,
            dst_ref=all_ref.at[me],
            send_sem=send_sem.at[step],
            recv_sem=recv_sem.at[step],
            device_id=(other(step), core),
            device_id_type=MESH,
        )

    def send(step, carry):
        ids_copy(step).start()
        return carry

    lax.fori_loop(1, holders, send, 0)
    with jax.named_scope("kv1"):
        lax.fori_loop(first, pieces, project, 0)

    def finish(step, carry):
        ids_copy(step).wait()
        return carry

    with jax.named_scope("ids"):
        lax.fori_loop(1, holders, finish, 0)
    with jax.named_scope("tables"):
        plan_tables(holders, planes, reads, pass_dev, most, variants, all_ref, tab_ref)


def project(planes, most, variants, ids, store, store_gain, w_key, w_value):
    holders = lax.axis_size("st")
    pass_dev, length, model = store.shape
    pieces = math.gcd(pass_dev, 6)
    width = w_key.shape[1]
    table_rows = 8 + -(-planes * most // 8) * 8
    return pl.pallas_call(
        functools.partial(project_kernel, holders, planes, pieces, most, variants),
        out_shape=(
            jax.ShapeDtypeStruct((table_rows, 128), jnp.int32),
            jax.ShapeDtypeStruct((pass_dev, length, 2 * width), BF16),
        ),
        in_specs=[VMEM, ANY, VMEM, VMEM, VMEM],
        out_specs=(VMEM, VMEM),
        scratch_shapes=[
            pltpu.VMEM((pass_dev * length, model), BF16),
            pltpu.VMEM((8, 128), jnp.int32),
            pltpu.VMEM((holders, 8, 128), jnp.int32),
            pltpu.SemaphoreType.DMA((pieces,)),
            pltpu.SemaphoreType.DMA((holders,)),
            pltpu.SemaphoreType.DMA((holders,)),
        ],
        compiler_params=pltpu.CompilerParams(collective_id=0, has_side_effects=True, vmem_limit_bytes=LIMIT),
        cost_estimate=pl.CostEstimate(
            flops=4 * pass_dev * length * model * width, bytes_accessed=store.size * 2, transcendentals=0
        ),
    )(ids, store.reshape(pass_dev * length, model), store_gain.reshape(1, model), w_key, w_value)


def chunks_of(caps):
    cut = [(0, caps[0] // 2, 1), (caps[0] // 2, caps[0], 1)]
    for k in range(1, len(caps)):
        if caps[k] > caps[k - 1]:
            cut.append((caps[k - 1], caps[k], k + 1))
    return cut


def mixer_kernel(
    planes,
    caps,
    most,
    block_len,
    per_block,
    tab,
    scale_ref,
    gain_ref,
    mix_ref,
    kv_hbm,
    hidden_hbm,
    w_pool_hbm,
    w_query_hbm,
    w_gate_hbm,
    w_branch_hbm,
    w_out_hbm,
    out_ref,
    kv,
    normed,
    w_pool,
    w_query,
    w_gate,
    w_branch,
    w_branch_far,
    w_out,
    w_out_far,
    pool_in,
    pool_out,
    pool_far,
    branch,
    gate,
    query,
    read,
    read_far,
    own_lists,
    *rest,
):
    reach = planes - 1
    lists = [rest[w * reach : (w + 1) * reach] for w in range(2)]
    picked, final, load_sem, z_send, z_recv, in_send, in_recv, core_send, core_recv = rest[2 * reach :]
    holders = lax.axis_size("st")
    side = holders // planes
    me = lax.axis_index("st")
    core = lax.axis_index("tp")
    z, c = lax.div(me, side), lax.rem(me, side)
    tokens, model = normed.shape
    half = out_ref.shape[1]
    cuts = chunks_of(caps)
    beyond = (planes - 1 - z, z)
    behind = (z, planes - 1 - z)
    step_to = (side, -side)

    mine = pl.ds(pl.multiple_of(core * half, half), half)
    theirs = pl.ds(pl.multiple_of((1 - core) * half, half), half)
    loads = [
        pltpu.make_async_copy(src, dst, load_sem.at[i])
        for i, (src, dst) in enumerate(
            (
                (kv_hbm, kv),
                (hidden_hbm, normed),
                (w_pool_hbm, w_pool),
                (w_query_hbm, w_query),
                (w_branch_hbm.at[:, mine], w_branch),
                (w_gate_hbm, w_gate),
                (w_out_hbm.at[:, mine], w_out),
            )
        )
    ]
    for copy in loads:
        copy.start()

    barrier = pltpu.get_barrier_semaphore()

    def greet(device):
        pl.semaphore_signal(barrier, inc=1, device_id=device, device_id_type=MESH)

    plane_mates = [z * side + lax.rem(c + rel, side) for rel in range(1, side)]
    for mate in plane_mates:
        greet((mate, core))
    greet((me, 1 - core))
    for way in range(2):
        pl.when(beyond[way] >= 1)(lambda way=way: greet((me + step_to[way], core)))
    with jax.named_scope("greet"):
        pl.semaphore_wait(barrier, side + (z + reach - 1) // reach + (beyond[0] + reach - 1) // reach)

    def partner(src, dst, i):
        return pltpu.make_async_remote_copy(
            src_ref=src,
            dst_ref=dst,
            send_sem=core_send.at[i],
            recv_sem=core_recv.at[i],
            device_id=(me, 1 - core),
            device_id_type=MESH,
        )

    weight_swaps = [
        partner(w_branch_hbm.at[:, theirs], w_branch_far, 0),
        partner(w_out_hbm.at[:, theirs], w_out_far, 1),
    ]
    pool_swap = partner(pool_out, pool_far, 2)

    def hop(way, d, i):
        first, last, _ = cuts[i]
        src = own_lists.at[way] if d == 0 else lists[way][d - 1]
        return pltpu.make_async_remote_copy(
            src_ref=src.at[pl.ds(first, last - first)],
            dst_ref=lists[way][d].at[pl.ds(first, last - first)],
            send_sem=z_send.at[way, d, i],
            recv_sem=z_recv.at[way, d, i],
            device_id=(me + step_to[way], core),
            device_id_type=MESH,
        )

    def arrive(way, d, i):
        first, last, _ = cuts[i]
        ref = lists[way][d - 1].at[pl.ds(first, last - first)]
        pltpu.make_async_remote_copy(
            src_ref=ref,
            dst_ref=ref,
            send_sem=z_send.at[way, d - 1, i],
            recv_sem=z_recv.at[way, d - 1, i],
            device_id=(me, 1 - core),
            device_id_type=MESH,
        ).wait_recv()

    def forward(d, i):
        need = cuts[i][2]
        if need > reach - d:
            return
        for way in range(2):

            def go(way=way):
                arrive(way, d, i)
                hop(way, d, i).start()

            pl.when((behind[way] >= d) & (beyond[way] >= need))(go)

    def keep(d):
        for i, (_, _, need) in enumerate(cuts):
            if need > reach - d + 1:
                continue
            for way in range(2):
                pl.when((behind[way] >= d) & (beyond[way] + 1 == need))(lambda way=way, i=i: arrive(way, d, i))


    def spread_copy(rel, q):
        mate = z * side + lax.rem(c + rel, side)
        return pltpu.make_async_remote_copy(
            src_ref=picked.at[rel - 1, pl.ds(q * most, most)],
            dst_ref=final.at[pl.ds((c * planes + q) * most, most)],
            send_sem=in_send.at[rel - 1, q],
            recv_sem=in_recv.at[c * planes + q],
            device_id=(mate, core),
            device_id_type=MESH,
        )

    def spread(src, q):
        for rel in range(1, side):
            mate = lax.rem(c + rel, side)
            for j in range(most):
                picked[rel - 1, q * most + j] = src[tab[8 + q * most + j, mate]]
        for rel in range(1, side):
            spread_copy(rel, q).start()
        for j in range(most):
            final[(c * planes + q) * most + j] = src[tab[8 + q * most + j, c]]

    def spread_from(d):
        for way in range(2):
            q = z - d if way == 0 else z + d
            pl.when(behind[way] >= d)(lambda way=way, q=q: spread(lists[way][d - 1], q))

    with jax.named_scope("first_sends"):
        loads[0].wait()
        for way in range(2):
            for s in range(caps[-1]):
                own_lists[way, s] = kv[tab[way, s]]
        for i, (_, _, need) in enumerate(cuts):
            for way in range(2):
                pl.when(beyond[way] >= need)(lambda way=way, i=i: hop(way, 0, i).start())
        spread(kv, z)
        for copy in weight_swaps:
            copy.start()

    def norm(lo, hi, rows=32):
        def body(i, carry):
            at = pl.ds(pl.multiple_of(i * rows, rows), rows)
            normed[at, :] = rms_rows(normed[at, :].astype(F32), gain_ref[...]).astype(BF16)
            return carry

        lax.fori_loop(lo // rows, hi // rows, body, 0)

    piece = math.gcd(tokens, 256)
    pieces = tokens // piece
    halo = pool_in.shape[0] - tokens
    groups, group_dim = mix_ref.shape[:2]

    def project_rows(lo, hi):
        def body(i, carry):
            at = pl.ds(pl.multiple_of(i * piece, piece), piece)
            rows = normed[at, :]
            pool_in[pl.ds(pl.multiple_of(halo + i * piece, halo), piece), :] = jnp.dot(
                rows, w_pool[...], preferred_element_type=F32
            ).astype(BF16)
            query[at, :] = jnp.dot(rows, w_query[...], preferred_element_type=F32).astype(BF16)
            return carry

        lax.fori_loop(lo, hi, body, 0)

    def pool_rows(i, carry):
        at = pl.ds(pl.multiple_of(i * piece, piece), piece)
        position = i * piece + lax.broadcasted_iota(jnp.int32, (piece, 1), 0)
        for g in range(groups):
            cols = slice(g * group_dim, (g + 1) * group_dim)
            wide = pool_in[pl.ds(pl.multiple_of(i * piece, piece), piece + halo), cols].astype(F32)
            sums = []
            total = wide
            shift = 1
            while shift < halo:
                total = total + pltpu.roll(total, shift, 0)
                sums.append(total[halo:])
                shift *= 2
            per_core = [sums[k * groups + g] for k in range(len(sums) // groups)]
            level = per_core[0]
            window = 2 ** (g + 1)
            for k in range(1, len(per_core)):
                level = jnp.where(core == k, per_core[k], level)
                window = jnp.where(core == k, 2 ** (k * groups + g + 1), window)
            count = jnp.minimum(position + 1, window).astype(F32)
            pooled = (level / count - wide[halo:]).astype(BF16)
            pool_out[at, cols] = jnp.dot(pooled, mix_ref[g], preferred_element_type=F32).astype(BF16)
        return carry

    def gate_rows(lo, hi):
        def body(i, carry):
            at = pl.ds(pl.multiple_of(i * piece, piece), piece)
            for j in range(2):
                cols = slice(j * half // 2, (j + 1) * half // 2)
                logits = jnp.dot(normed[at, :], w_gate[:, cols], preferred_element_type=F32)
                gate[at, cols] = 1.0 / (1.0 + jnp.exp(-logits))
            return carry

        lax.fori_loop(lo, hi, body, 0)

    def two_terms(a, w, a_far, w_far):
        near = jnp.dot(a, w, preferred_element_type=F32).astype(BF16).astype(F32)
        far = jnp.dot(a_far, w_far, preferred_element_type=F32).astype(BF16).astype(F32)
        return near + far

    def branch_rows(i, carry):
        at = pl.ds(pl.multiple_of(i * piece, piece), piece)
        for j in range(2):
            cols = slice(j * half // 2, (j + 1) * half // 2)
            branch[at, cols] = two_terms(
                pool_out[at, :], w_branch[:, cols], pool_far[at, :], w_branch_far[:, cols]
            )
        return carry

    def forward_all(d, which):
        for i in which:
            if i < len(cuts):
                forward(d, i)

    with jax.named_scope("norm"):
        loads[1].wait()
        norm(0, tokens)
    with jax.named_scope("project"):
        loads[2].wait()
        loads[3].wait()
        pool_in[:halo, :] = jnp.zeros((halo, pool_in.shape[1]), BF16)
        project_rows(0, pieces)
    with jax.named_scope("pool"):
        forward_all(1, [0])
        lax.fori_loop(0, pieces, pool_rows, 0)
        pool_swap.start()
    with jax.named_scope("gate"):
        loads[5].wait()
        gate_rows(0, pieces // 2)
        forward_all(1, [1])
        gate_rows(pieces // 2, pieces)
    with jax.named_scope("branch"):
        loads[4].wait()
        loads[6].wait()
        for copy in weight_swaps:
            copy.wait()
        pool_swap.wait()
        lax.fori_loop(0, pieces, branch_rows, 0)
    with jax.named_scope("spread1"):
        forward_all(1, range(2, len(cuts)))
        keep(1)
        spread_from(1)
    for d in range(2, planes):
        with jax.named_scope(f"spread{d}"):
            if d < planes - 1:
                forward_all(d, range(len(cuts)))
            keep(d)
            spread_from(d)

    with jax.named_scope("arrivals"):
        for rel in range(1, side):
            source = lax.rem(c + side - rel, side)
            for q in range(planes):
                at = pl.ds((source * planes + q) * most, most)
                pltpu.make_async_remote_copy(
                    src_ref=final.at[at],
                    dst_ref=final.at[at],
                    send_sem=in_send.at[rel - 1, q],
                    recv_sem=in_recv.at[source * planes + q],
                    device_id=(me, 1 - core),
                    device_id_type=MESH,
                ).wait_recv()

    blocks = tokens // block_len
    heads = scale_ref.shape[0]
    width = query.shape[1]
    head_dim = width // heads
    reads = blocks * per_block
    slot_base = lax.rem(c, 128 // reads) * reads

    def read_swap(b):
        at = pl.ds(pl.multiple_of(b * block_len, block_len), block_len)
        return partner(read.at[at], read_far.at[at], 3 + b)

    def attend_block(b):
        at = pl.ds(pl.multiple_of(b * block_len, block_len), block_len)
        memory = jnp.concatenate(
            [final[tab[2, slot_base + b * per_block + i]] for i in range(per_block)], axis=0
        )
        for h in range(heads):
            cut = slice(h * head_dim, (h + 1) * head_dim)
            scale = scale_ref[h] * (1.0 / math.sqrt(head_dim))
            scores = lax.dot_general(
                query[at, cut], memory[:, cut], (((1,), (1,)), ((), ())), preferred_element_type=F32
            )
            scores = scores * scale
            top = jnp.exp(scores - jnp.max(scores, axis=-1, keepdims=True))
            weights = (top * (1.0 / jnp.sum(top, axis=-1, keepdims=True))).astype(BF16)
            read[at, cut] = jnp.dot(
                weights, memory[:, width + h * head_dim : width + (h + 1) * head_dim], preferred_element_type=F32
            ).astype(BF16)

    unroll = math.gcd(blocks, 4)

    def attend(i, carry):
        for k in range(unroll):
            attend_block(i * unroll + k)
        for k in range(unroll):
            read_swap(i * unroll + k).start()
        return carry

    with jax.named_scope("attend"):
        lax.fori_loop(0, blocks // unroll, attend, 0)

    def finish(b, carry):
        at = pl.ds(pl.multiple_of(b * block_len, block_len), block_len)
        read_swap(b).wait()
        for j in range(2):
            cols = slice(j * half // 2, (j + 1) * half // 2)
            terms = two_terms(read[at, :], w_out[:, cols], read_far[at, :], w_out_far[:, cols])
            out_ref[at, cols] = (branch[at, cols] + gate[at, cols] * terms).astype(BF16)
        return carry

    with jax.named_scope("finish"):
        lax.fori_loop(0, blocks, finish, 0)

    for way in range(2):
        for i, (_, _, need) in enumerate(cuts):
            for d in range(reach - need + 1):
                pl.when((behind[way] >= d) & (beyond[way] >= need))(
                    lambda way=way, d=d, i=i: hop(way, d, i).wait_send()
                )
    for rel in range(1, side):
        for q in range(planes):
            spread_copy(rel, q).wait_send()


def mixer(planes, most, block_len, per_block, caps, collective_id, *operands):
    tab, scale, gain, mix, kv, hidden, w_pool, w_query, w_gate, w_branch, w_out = operands
    holders = lax.axis_size("st")
    side = holders // planes
    reach = planes - 1
    tokens, model = hidden.shape
    half = w_gate.shape[1]
    pool_width, width = w_pool.shape[1], w_query.shape[1]
    slot = kv.shape[1:]
    cores = lax.axis_size("tp")
    halo = 2 ** (cores * mix.shape[0])
    nch = len(chunks_of(caps))
    blocks = tokens // block_len
    v = pltpu.VMEM
    dma = pltpu.SemaphoreType.DMA
    flops = 2 * tokens * (model * (pool_width + width + half) + 2 * (pool_width + width) * half)
    return pl.pallas_call(
        functools.partial(mixer_kernel, planes, caps, most, block_len, per_block),
        out_shape=jax.ShapeDtypeStruct((tokens, half), BF16),
        in_specs=[SMEM, SMEM, VMEM, VMEM] + [ANY] * 7,
        out_specs=VMEM,
        scratch_shapes=[
            v(kv.shape, BF16),
            v(hidden.shape, BF16),
            v(w_pool.shape, BF16),
            v(w_query.shape, BF16),
            v(w_gate.shape, BF16),
            v((pool_width, half), BF16),
            v((pool_width, half), BF16),
            v((width, half), BF16),
            v((width, half), BF16),
            v((tokens + halo, pool_width), BF16),
            v((tokens, pool_width), BF16),
            v((tokens, pool_width), BF16),
            v((tokens, half), F32),
            v((tokens, half), F32),
            v((tokens, width), BF16),
            v((tokens, width), BF16),
            v((tokens, width), BF16),
            v((2, caps[-1], *slot), BF16),
            *[v((caps[reach - d], *slot), BF16) for _ in range(2) for d in range(1, planes)],
            v((side - 1, planes * most, *slot), BF16),
            v((holders * most, *slot), BF16),
            dma((7,)),
            dma((2, reach, nch)),
            dma((2, reach, nch)),
            dma((side - 1, planes)),
            dma((holders,)),
            dma((3 + blocks,)),
            dma((3 + blocks,)),
        ],
        compiler_params=pltpu.CompilerParams(
            collective_id=collective_id, has_side_effects=True, vmem_limit_bytes=LIMIT
        ),
        cost_estimate=pl.CostEstimate(flops=flops, bytes_accessed=32 * 2**20, transcendentals=0),
    )(*operands)


def body(
    planes,
    hidden,
    norm_gain,
    store,
    store_gain,
    passage_ids,
    w_pool,
    pool_mix,
    w_branch,
    w_query,
    w_key,
    w_value,
    sharpness,
    w_out,
    w_gate,
):
    holders = lax.axis_size("st")
    side = holders // planes
    blocks, per_block = passage_ids.shape
    reads = blocks * per_block
    pass_dev = store.shape[0]
    tokens, model = hidden.shape
    most = max(1, 2 * reads // holders)

    one = min(pass_dev, side * most)
    full = tuple(min(pass_dev, k * one) for k in range(1, planes))
    variants = []
    for sixteenths in (9, 10, 11):
        first = one * sixteenths // 16
        lengths = (first, first + pass_dev // 6, first + pass_dev // 4)[: planes - 1]
        variants.append(tuple(map(min, lengths, full)))
    variants = (*variants, full)
    tab, own_kv = project(planes, most, variants, passage_ids, store, store_gain, w_key, w_value)
    operands = (
        tab,
        sharpness,
        norm_gain.reshape(1, model),
        pool_mix,
        own_kv,
        hidden,
        w_pool,
        w_query,
        w_gate,
        w_branch,
        w_out,
    )
    run = functools.partial(mixer, planes, most, tokens // blocks, per_block)
    return lax.switch(
        tab[3, 0], [functools.partial(run, caps, i + 1) for i, caps in enumerate(variants)], *operands
    )


def solution(mesh):
    placed = (
        P("st", None),
        P(),
        P("st", None, None),
        P(),
        P("st", None),
        P(None, "tp"),
        P("tp", None, None),
        P("tp", None),
        P(None, "tp"),
        P(None, "tp"),
        P(None, "tp"),
        P("tp"),
        P("tp", None),
        P(None, "tp"),
    )
    return jax.shard_map(
        functools.partial(body, planes_of(mesh)), mesh=mesh, in_specs=placed, out_specs=P("st", "tp"), check_vma=False
    )
```

```python
import functools
import math

import jax
import jax.numpy as jnp
from jax import lax
from jax.experimental import pallas as pl
from jax.experimental.pallas import tpu as pltpu
from jax.sharding import PartitionSpec as P

MESH = pl.DeviceIdType.MESH
F32 = jnp.float32
BF16 = jnp.bfloat16
ANY = pl.BlockSpec(memory_space=pl.ANY)
VMEM = pl.BlockSpec(memory_space=pltpu.VMEM)
SMEM = pl.BlockSpec(memory_space=pltpu.SMEM)
LIMIT = 66_000_000


def planes_of(mesh):
    heights = {getattr(d, "coords", (0, 0, 0))[2] for d in mesh.devices.flat}
    return len(heights)


def rms_rows(wide, gain):
    scale = lax.rsqrt(jnp.mean(wide * wide, axis=-1, keepdims=True) + 1e-05)
    return wide * scale * gain


def plan_tables(holders, planes, reads, pass_dev, most, variants, all_ref, tab_ref):
    side = holders // planes
    lanes = 128
    per = lanes // reads
    me = lax.axis_index("st")
    z, c = lax.div(me, side), lax.rem(me, side)

    def lane_of(rows):
        return lax.broadcasted_iota(jnp.int32, (rows, lanes), 1).astype(F32)

    def sub_of(rows, width=lanes):
        return lax.broadcasted_iota(jnp.int32, (rows, width), 0).astype(F32)

    def whole(x, by):
        return jnp.floor((x + 0.5) * (1.0 / by))

    segment = whole(lane_of(1), reads)

    def requests(plane):
        return [requests_row(all_ref, plane, side, per, r, segment) for r in range(side // per)]

    holder_at = lax.broadcasted_iota(jnp.int32, (1, holders), 1).astype(F32)
    plane_at = whole(holder_at, side)
    far_up = jnp.zeros((pass_dev, holders), F32)
    far_down = jnp.zeros((pass_dev, holders), F32)
    near_up = jnp.zeros((pass_dev, holders), F32)
    near_down = jnp.zeros((pass_dev, holders), F32)
    for p in range(planes):
        hits = jnp.zeros((pass_dev, holders), F32)
        for row in requests(p):
            owner = whole(row, pass_dev)
            inside = row - owner * pass_dev
            a = jnp.where(inside == sub_of(pass_dev), 1.0, 0.0).astype(BF16)
            b = jnp.where(owner == sub_of(holders), 1.0, 0.0).astype(BF16)
            hits = hits + lax.dot_general(a, b, (((1,), (1,)), ((), ())), preferred_element_type=F32)
        ahead = jnp.where(hits > 0.5, p - plane_at, 0.0)
        far_up = jnp.maximum(far_up, ahead)
        far_down = jnp.maximum(far_down, -ahead)
        near_up = jnp.where(ahead == 1.0, 1.0, near_up)
        near_down = jnp.where(ahead == -1.0, 1.0, near_down)

    longest = [jnp.zeros((1, holders), F32) for _ in range(planes - 2)]
    for reach, edge in ((near_up, 0), (near_down, planes - 1)):
        count = jnp.sum(reach, axis=0, keepdims=True)
        longest[0] = jnp.maximum(longest[0], jnp.where(plane_at == edge, count, 0.0))
    for reach, left in ((far_up, planes - 1 - plane_at), (far_down, plane_at)):
        for d in range(1, planes):
            count = jnp.sum(jnp.where(reach >= d, 1.0, 0.0), axis=0, keepdims=True)
            for k in range(planes - 2):
                longest[k] = jnp.maximum(longest[k], jnp.where(left - d == k, count, 0.0))
    longest = [jnp.max(x, axis=1, keepdims=True) for x in longest]
    variant = jnp.zeros((1, 1), F32)
    for caps in variants[:-1]:
        over = jnp.zeros((1, 1), F32)
        for k, room in enumerate(caps):
            over = jnp.maximum(over, jnp.where(longest[k] > room, 1.0, 0.0))
        variant = variant + over

    lower = lax.broadcasted_iota(jnp.int32, (pass_dev, pass_dev), 1) < lax.broadcasted_iota(
        jnp.int32, (pass_dev, pass_dev), 0
    )
    diagonal = lax.broadcasted_iota(jnp.int32, (pass_dev, pass_dev), 1) == lax.broadcasted_iota(
        jnp.int32, (pass_dev, pass_dev), 0
    )

    def place_in(reach, q):
        col = jnp.sum(jnp.where(holder_at == (q * side + c).astype(F32), reach, 0.0), axis=1, keepdims=True)
        row = jnp.sum(jnp.where(diagonal, col, 0.0), axis=0, keepdims=True)
        before = (row > col) | ((row == col) & lower)
        return jnp.sum(jnp.where(before, 1.0, 0.0), axis=1, keepdims=True)

    number = sub_of(pass_dev)
    orders = [
        jnp.sum(jnp.where(place_in(reach, z) == lane_of(pass_dev), number, 0.0), axis=0, keepdims=True)
        for reach in (far_up, far_down, jnp.where(z == 0, near_up, near_down))
    ]
    where_at = []
    for q in range(planes):
        reach = jnp.where(q < z, far_up, far_down)
        if q == 0:
            reach = jnp.where(z == 1, near_up, reach)
        if q == planes - 1:
            reach = jnp.where(z == planes - 2, near_down, reach)
        place = place_in(reach, jnp.int32(q))
        where_at.append(jnp.where(q == z, sub_of(pass_dev, 1), place))

    square_sub = sub_of(lanes)
    square_lane = lane_of(lanes)
    close = (square_sub < square_lane) & (whole(square_sub, reads) == whole(square_lane, reads))
    picks = jnp.zeros((planes * most, lanes), F32)
    slots = jnp.zeros((1, lanes), F32)
    for r, row in enumerate(requests(z)):
        owner = whole(row, pass_dev)
        inside = row - owner * pass_dev
        owner_col = jnp.sum(jnp.where(square_sub == square_lane, owner, 0.0), axis=1, keepdims=True)
        rank = jnp.sum(jnp.where(close & (owner_col == owner), 1.0, 0.0), axis=0, keepdims=True)
        of_plane = whole(owner, side)
        of_side = owner - of_plane * side
        here = of_side == c.astype(F32)
        found = jnp.zeros((1, lanes), F32)
        for q in range(planes):
            hit = here & (of_plane == q) & (inside == number)
            found = found + jnp.sum(jnp.where(hit, where_at[q], 0.0), axis=0, keepdims=True)
        target = jnp.where(here, of_plane * most + rank, -1.0)
        values = jnp.where(target == sub_of(planes * most), found, 0.0)
        for t in range(per):
            column = jnp.sum(jnp.where(segment == t, values, 0.0), axis=1, keepdims=True)
            picks = jnp.where(lane_of(planes * most) == r * per + t, column, picks)
        slots = jnp.where(lax.div(c, per) == r, (of_side * planes + of_plane) * most + rank, slots)
    for i, row in enumerate((*orders[:2], slots, variant + jnp.zeros((1, lanes), F32), orders[2])):
        tab_ref[i : i + 1, :] = row.astype(jnp.int32)
    tab_ref[8 : 8 + planes * most, :] = picks.astype(jnp.int32)


def requests_row(all_ref, plane, side, per, r, segment):
    row = jnp.zeros(segment.shape, F32)
    for t in range(per):
        ids = all_ref[plane * side + r * per + t][0:1, :].astype(F32)
        row = jnp.where(segment == t, ids, row)
    return row


def project_kernel(
    holders,
    planes,
    pieces,
    most,
    variants,
    ids_ref,
    store_ref,
    gain_ref,
    wk_hbm,
    wv_hbm,
    tab_ref,
    kv_ref,
    rows,
    wk_ref,
    wv_ref,
    mine_ids,
    all_ref,
    load_sem,
    send_sem,
    recv_sem,
):
    me = lax.axis_index("st")
    core = lax.axis_index("tp")
    piece = rows.shape[0] // pieces
    width = wk_ref.shape[1]
    pass_dev, length, _ = kv_ref.shape
    passages = piece // length
    per_block, blocks = ids_ref.shape
    reads = blocks * per_block
    weights = [
        pltpu.make_async_copy(src, dst, load_sem.at[pieces + i])
        for i, (src, dst) in enumerate(((wk_hbm, wk_ref), (wv_hbm, wv_ref)))
    ]

    def load(i):
        return pltpu.make_async_copy(
            store_ref.at[pl.ds(i * piece, piece)], rows.at[pl.ds(i * piece, piece)], load_sem.at[i]
        )

    load(0).start()
    for copy in weights:
        copy.start()
    for i in range(1, pieces):
        load(i).start()

    barrier = pltpu.get_barrier_semaphore()

    def other(step):
        return lax.rem(me + step, holders)

    def greet(step, carry):
        pl.semaphore_signal(barrier, inc=1, device_id=(other(step), core), device_id_type=MESH)
        return carry

    lax.fori_loop(1, holders, greet, 0)

    lane = lax.broadcasted_iota(jnp.int32, (per_block, 128), 1).astype(F32)
    lane = lane - reads * jnp.floor((lane + 0.5) * (1.0 / reads))
    block = jnp.floor((lane + 0.5) * (1.0 / per_block))
    inner = lane - block * per_block
    spread_ids = jnp.zeros((per_block, 128), F32)
    for k in range(blocks):
        spread_ids = jnp.where(block == k, ids_ref[:, k : k + 1].astype(F32), spread_ids)
    at_inner = lax.broadcasted_iota(jnp.int32, (per_block, 128), 0).astype(F32) == inner
    row = jnp.sum(jnp.where(at_inner, spread_ids, 0.0), axis=0, keepdims=True)
    mine_ids[...] = jnp.broadcast_to(row, mine_ids.shape).astype(jnp.int32)
    all_ref[me] = jnp.broadcast_to(row, mine_ids.shape).astype(jnp.int32)

    def project(i, carry):
        load(i).wait()
        start = pl.multiple_of(i * piece, piece)
        normed = rms_rows(rows[pl.ds(start, piece), :].astype(F32), gain_ref[...]).astype(BF16)
        for half, w_ref in enumerate((wk_ref, wv_ref)):
            part = jnp.dot(normed, w_ref[...], preferred_element_type=F32).astype(BF16)
            kv_ref[pl.ds(i * passages, passages), :, half * width : (half + 1) * width] = part.reshape(
                passages, length, width
            )
        return carry

    first = 1
    for copy in weights:
        copy.wait()
    with jax.named_scope("kv0"):
        lax.fori_loop(0, first, project, 0)
    with jax.named_scope("greet_all"):
        pl.semaphore_wait(barrier, holders - 1)

    def ids_copy(step):
        return pltpu.make_async_remote_copy(
            src_ref=mine_ids,
            dst_ref=all_ref.at[me],
            send_sem=send_sem.at[0],
            recv_sem=recv_sem.at[0],
            device_id=(other(step), core),
            device_id_type=MESH,
        )

    def send(step, carry):
        ids_copy(step).start()
        return carry

    lax.fori_loop(1, holders, send, 0)
    with jax.named_scope("kv1"):
        lax.fori_loop(first, pieces, project, 0)

    every = all_ref.at[pl.ds(0, holders - 1)]
    with jax.named_scope("ids"):
        pltpu.make_async_remote_copy(
            src_ref=every,
            dst_ref=every,
            send_sem=send_sem.at[0],
            recv_sem=recv_sem.at[0],
            device_id=(other(1), core),
            device_id_type=MESH,
        ).wait()
    with jax.named_scope("tables"):
        plan_tables(holders, planes, reads, pass_dev, most, variants, all_ref, tab_ref)


def project(planes, most, variants, ids, store, store_gain, w_key, w_value):
    holders = lax.axis_size("st")
    pass_dev, length, model = store.shape
    pieces = math.gcd(pass_dev, 6)
    width = w_key.shape[1]
    table_rows = 8 + -(-planes * most // 8) * 8
    return pl.pallas_call(
        functools.partial(project_kernel, holders, planes, pieces, most, variants),
        out_shape=(
            jax.ShapeDtypeStruct((table_rows, 128), jnp.int32),
            jax.ShapeDtypeStruct((pass_dev, length, 2 * width), BF16),
        ),
        in_specs=[VMEM, ANY, VMEM, ANY, ANY],
        out_specs=(VMEM, VMEM),
        scratch_shapes=[
            pltpu.VMEM((pass_dev * length, model), BF16),
            pltpu.VMEM(w_key.shape, BF16),
            pltpu.VMEM(w_value.shape, BF16),
            pltpu.VMEM((8, 128), jnp.int32),
            pltpu.VMEM((holders, 8, 128), jnp.int32),
            pltpu.SemaphoreType.DMA((pieces + 2,)),
            pltpu.SemaphoreType.DMA((1,)),
            pltpu.SemaphoreType.DMA((1,)),
        ],
        compiler_params=pltpu.CompilerParams(collective_id=0, has_side_effects=True, vmem_limit_bytes=LIMIT),
        cost_estimate=pl.CostEstimate(
            flops=4 * pass_dev * length * model * width, bytes_accessed=store.size * 2, transcendentals=0
        ),
    )(ids.T, store.reshape(pass_dev * length, model), store_gain.reshape(1, model), w_key, w_value)


def chunks_of(caps):
    cut = [(0, caps[0] // 2, 1), (caps[0] // 2, caps[0], 1)]
    for k in range(1, len(caps)):
        if caps[k] > caps[k - 1]:
            cut.append((caps[k - 1], caps[k], k + 1))
    return cut


def mixer_kernel(
    planes,
    caps,
    most,
    block_len,
    per_block,
    tab,
    scale_ref,
    gain_ref,
    mix_ref,
    kv_hbm,
    hidden_hbm,
    w_pool_hbm,
    w_query_hbm,
    w_gate_hbm,
    w_branch_hbm,
    w_out_hbm,
    out_ref,
    kv,
    normed,
    w_pool,
    w_query,
    w_gate,
    w_branch,
    w_branch_far,
    w_out,
    w_out_far,
    pool_in,
    pool_out,
    pool_far,
    branch,
    gate,
    query,
    read,
    read_far,
    own_lists,
    *rest,
):
    reach = planes - 1
    lists = [rest[w * reach : (w + 1) * reach] for w in range(2)]
    near_own, near_up, near_down, picked, final, out_rows, load_sem, out_sem, near_send, near_recv, z_send, z_recv, in_send, in_recv, core_send, core_recv = rest[2 * reach :]
    holders = lax.axis_size("st")
    side = holders // planes
    me = lax.axis_index("st")
    core = lax.axis_index("tp")
    z, c = lax.div(me, side), lax.rem(me, side)
    tokens, model = normed.shape
    half = out_rows.shape[1]
    near = (near_up, near_down)
    cuts = chunks_of(caps)
    beyond = (planes - 1 - z, z)
    behind = (z, planes - 1 - z)
    step_to = (side, -side)

    mine = pl.ds(pl.multiple_of(core * half, half), half)
    theirs = pl.ds(pl.multiple_of((1 - core) * half, half), half)
    loads = [
        pltpu.make_async_copy(src, dst, load_sem.at[i])
        for i, (src, dst) in enumerate(
            (
                (kv_hbm, kv),
                (hidden_hbm, normed),
                (w_pool_hbm, w_pool),
                (w_query_hbm, w_query),
                (w_branch_hbm.at[:, mine], w_branch),
                (w_gate_hbm, w_gate),
                (w_out_hbm.at[:, mine], w_out),
            )
        )
    ]
    for copy in loads:
        copy.start()

    barrier = pltpu.get_barrier_semaphore()

    def greet(device):
        pl.semaphore_signal(barrier, inc=1, device_id=device, device_id_type=MESH)

    plane_mates = [z * side + lax.rem(c + rel, side) for rel in range(1, side)]
    for mate in plane_mates:
        greet((mate, core))
    greet((me, 1 - core))
    for way in range(2):
        pl.when(beyond[way] >= 1)(lambda way=way: greet((me + step_to[way], core)))
    with jax.named_scope("greet"):
        pl.semaphore_wait(barrier, side + (z + reach - 1) // reach + (beyond[0] + reach - 1) // reach)

    def partner(src, dst, i):
        return pltpu.make_async_remote_copy(
            src_ref=src,
            dst_ref=dst,
            send_sem=core_send.at[i],
            recv_sem=core_recv.at[i],
            device_id=(me, 1 - core),
            device_id_type=MESH,
        )

    weight_swaps = [
        partner(w_branch_hbm.at[:, theirs], w_branch_far, 0),
        partner(w_out_hbm.at[:, theirs], w_out_far, 1),
    ]
    pool_swap = partner(pool_out, pool_far, 2)

    def hop(way, d, i):
        first, last, _ = cuts[i]
        src = own_lists.at[way] if d == 0 else lists[way][d - 1]
        return pltpu.make_async_remote_copy(
            src_ref=src.at[pl.ds(first, last - first)],
            dst_ref=lists[way][d].at[pl.ds(first, last - first)],
            send_sem=z_send.at[way, d, i],
            recv_sem=z_recv.at[way, d, i],
            device_id=(me + step_to[way], core),
            device_id_type=MESH,
        )

    def arrive(way, d, i):
        first, last, _ = cuts[i]
        ref = lists[way][d - 1].at[pl.ds(first, last - first)]
        pltpu.make_async_remote_copy(
            src_ref=ref,
            dst_ref=ref,
            send_sem=z_send.at[way, d - 1, i],
            recv_sem=z_recv.at[way, d - 1, i],
            device_id=(me, 1 - core),
            device_id_type=MESH,
        ).wait_recv()

    def near_hop(way):
        return pltpu.make_async_remote_copy(
            src_ref=near_own,
            dst_ref=near[way],
            send_sem=near_send.at[0],
            recv_sem=near_recv.at[way],
            device_id=(me + step_to[way], core),
            device_id_type=MESH,
        )

    def near_arrive(way):
        pltpu.make_async_remote_copy(
            src_ref=near[way],
            dst_ref=near[way],
            send_sem=near_send.at[0],
            recv_sem=near_recv.at[way],
            device_id=(me, 1 - core),
            device_id_type=MESH,
        ).wait_recv()

    def forward(d, i, here):
        need = cuts[i][2]
        if need > reach - d:
            return
        for way in range(2):

            def go(way=way):
                arrive(way, d, i)
                hop(way, d, i).start()

            pl.when(here(way) & (behind[way] >= d) & (beyond[way] >= need))(go)

    def keep(d, here):
        for i, (_, _, need) in enumerate(cuts):
            if need > reach - d + 1:
                continue
            for way in range(2):
                pl.when(here(way) & (behind[way] >= d) & (beyond[way] + 1 == need))(lambda way=way, i=i: arrive(way, d, i))


    def spread_copy(rel, q):
        mate = z * side + lax.rem(c + rel, side)
        return pltpu.make_async_remote_copy(
            src_ref=picked.at[rel - 1, pl.ds(q * most, most)],
            dst_ref=final.at[pl.ds((c * planes + q) * most, most)],
            send_sem=in_send.at[rel - 1, q],
            recv_sem=in_recv.at[c * planes + q],
            device_id=(mate, core),
            device_id_type=MESH,
        )

    def spread(src, q):
        for rel in range(1, side):
            mate = lax.rem(c + rel, side)
            for j in range(most):
                picked[rel - 1, q * most + j] = src[tab[8 + q * most + j, mate]]
        for rel in range(1, side):
            spread_copy(rel, q).start()
        for j in range(most):
            final[(c * planes + q) * most + j] = src[tab[8 + q * most + j, c]]

    def spread_from(d, here):
        for way in range(2):
            q = z - d if way == 0 else z + d
            pl.when(here(way) & (behind[way] >= d))(lambda way=way, q=q: spread(lists[way][d - 1], q))

    def spread_near():
        for way in range(2):

            def go(way=way):
                near_arrive(way)
                spread(near[way], z - 1 if way == 0 else z + 1)

            pl.when((behind[way] == 1) & (beyond[way] >= 1))(go)

    with jax.named_scope("first_sends"):
        loads[0].wait()
        for way in range(2):
            for s in range(caps[-1]):
                own_lists[way, s] = kv[tab[way, s]]
        for s in range(caps[0]):
            near_own[s] = kv[tab[4, s]]
        for way in range(2):
            pl.when(behind[way] == 0)(lambda way=way: near_hop(way).start())
        for i, (_, _, need) in enumerate(cuts):
            for way in range(2):
                pl.when(beyond[way] >= need)(lambda way=way, i=i: hop(way, 0, i).start())
        spread(kv, z)
        for copy in weight_swaps:
            copy.start()

    def norm(lo, hi, rows=32):
        def body(i, carry):
            at = pl.ds(pl.multiple_of(i * rows, rows), rows)
            normed[at, :] = rms_rows(normed[at, :].astype(F32), gain_ref[...]).astype(BF16)
            return carry

        lax.fori_loop(lo // rows, hi // rows, body, 0)

    piece = math.gcd(tokens, 256)
    pieces = tokens // piece
    halo = pool_in.shape[0] - tokens
    groups, group_dim = mix_ref.shape[:2]

    def project_rows(lo, hi):
        def body(i, carry):
            at = pl.ds(pl.multiple_of(i * piece, piece), piece)
            rows = normed[at, :]
            pool_in[pl.ds(pl.multiple_of(halo + i * piece, halo), piece), :] = jnp.dot(
                rows, w_pool[...], preferred_element_type=F32
            ).astype(BF16)
            query[at, :] = jnp.dot(rows, w_query[...], preferred_element_type=F32).astype(BF16)
            return carry

        lax.fori_loop(lo, hi, body, 0)

    def pool_rows(i, carry):
        at = pl.ds(pl.multiple_of(i * piece, piece), piece)
        position = i * piece + lax.broadcasted_iota(jnp.int32, (piece, 1), 0)
        for g in range(groups):
            cols = slice(g * group_dim, (g + 1) * group_dim)
            wide = pool_in[pl.ds(pl.multiple_of(i * piece, piece), piece + halo), cols].astype(F32)
            sums = []
            total = wide
            shift = 1
            while shift < halo:
                total = total + pltpu.roll(total, shift, 0)
                sums.append(total[halo:])
                shift *= 2
            per_core = [sums[k * groups + g] for k in range(len(sums) // groups)]
            level = per_core[0]
            window = 2 ** (g + 1)
            for k in range(1, len(per_core)):
                level = jnp.where(core == k, per_core[k], level)
                window = jnp.where(core == k, 2 ** (k * groups + g + 1), window)
            count = jnp.minimum(position + 1, window).astype(F32)
            pooled = (level / count - wide[halo:]).astype(BF16)
            pool_out[at, cols] = jnp.dot(pooled, mix_ref[g], preferred_element_type=F32).astype(BF16)
        return carry

    def gate_rows(lo, hi):
        def body(i, carry):
            at = pl.ds(pl.multiple_of(i * piece, piece), piece)
            for j in range(2):
                cols = slice(j * half // 2, (j + 1) * half // 2)
                logits = jnp.dot(normed[at, :], w_gate[:, cols], preferred_element_type=F32)
                gate[at, cols] = 1.0 / (1.0 + jnp.exp(-logits))
            return carry

        lax.fori_loop(lo, hi, body, 0)

    def two_terms(a, w, a_far, w_far):
        near = jnp.dot(a, w, preferred_element_type=F32).astype(BF16).astype(F32)
        far = jnp.dot(a_far, w_far, preferred_element_type=F32).astype(BF16).astype(F32)
        return near + far

    def branch_rows(i, carry):
        at = pl.ds(pl.multiple_of(i * piece, piece), piece)
        for j in range(2):
            cols = slice(j * half // 2, (j + 1) * half // 2)
            branch[at, cols] = two_terms(
                pool_out[at, :], w_branch[:, cols], pool_far[at, :], w_branch_far[:, cols]
            )
        return carry

    def at_edge(way):
        return beyond[way] == 0

    def inside(way):
        return beyond[way] >= 1

    def from_edge(way):
        return behind[way] == 1

    def from_inside(way):
        return behind[way] >= 2

    with jax.named_scope("norm"):
        loads[1].wait()
        norm(0, tokens)
    with jax.named_scope("project"):
        loads[2].wait()
        loads[3].wait()
        pool_in[:halo, :] = jnp.zeros((halo, pool_in.shape[1]), BF16)
        project_rows(0, pieces)
    with jax.named_scope("pool"):
        lax.fori_loop(0, pieces, pool_rows, 0)
        pool_swap.start()
    with jax.named_scope("step0"):
        forward(1, 0, from_inside)
    with jax.named_scope("gate"):
        loads[5].wait()
        gate_rows(0, pieces // 2)
    with jax.named_scope("step1"):
        forward(1, 1, from_inside)
        keep(1, at_edge)
        spread_from(1, at_edge)
        spread_near()
    with jax.named_scope("gate"):
        gate_rows(pieces // 2, pieces)
    with jax.named_scope("branch"):
        loads[4].wait()
        loads[6].wait()
        for copy in weight_swaps:
            copy.wait()
        pool_swap.wait()
        lax.fori_loop(0, pieces, branch_rows, 0)
    with jax.named_scope("step2"):
        for i in range(2, len(cuts)):
            forward(1, i, from_inside)
        keep(1, inside)
        spread_from(1, lambda way: inside(way) & from_inside(way))
        forward(1, 0, from_edge)
    for d in range(2, planes):
        with jax.named_scope(f"step{d + 1}"):
            forward(d, 0, inside)
            keep(d, at_edge)
            spread_from(d, at_edge)
            if d == 2:
                for i in range(1, len(cuts)):
                    forward(1, i, from_edge)
            for i in range(1, len(cuts)):
                forward(d, i, inside)
            keep(d, inside)
            spread_from(d, inside)

    with jax.named_scope("arrivals"):
        for rel in range(1, side):
            source = lax.rem(c + side - rel, side)
            for q in range(planes):
                at = pl.ds((source * planes + q) * most, most)
                pltpu.make_async_remote_copy(
                    src_ref=final.at[at],
                    dst_ref=final.at[at],
                    send_sem=in_send.at[rel - 1, q],
                    recv_sem=in_recv.at[source * planes + q],
                    device_id=(me, 1 - core),
                    device_id_type=MESH,
                ).wait_recv()

    blocks = tokens // block_len
    heads = scale_ref.shape[0]
    width = query.shape[1]
    head_dim = width // heads
    reads = blocks * per_block
    slot_base = lax.rem(c, 128 // reads) * reads

    def read_swap(b):
        at = pl.ds(pl.multiple_of(b * block_len, block_len), block_len)
        return partner(read.at[at], read_far.at[at], 3 + b)

    def attend_block(b):
        at = pl.ds(pl.multiple_of(b * block_len, block_len), block_len)
        memory = jnp.concatenate(
            [final[tab[2, slot_base + b * per_block + i]] for i in range(per_block)], axis=0
        )
        for h in range(heads):
            cut = slice(h * head_dim, (h + 1) * head_dim)
            scale = scale_ref[h] * (1.0 / math.sqrt(head_dim))
            scores = lax.dot_general(
                query[at, cut], memory[:, cut], (((1,), (1,)), ((), ())), preferred_element_type=F32
            )
            scores = scores * scale
            top = jnp.exp(scores - jnp.max(scores, axis=-1, keepdims=True))
            weights = (top * (1.0 / jnp.sum(top, axis=-1, keepdims=True))).astype(BF16)
            read[at, cut] = jnp.dot(
                weights, memory[:, width + h * head_dim : width + (h + 1) * head_dim], preferred_element_type=F32
            ).astype(BF16)

    unroll = math.gcd(blocks, 4)

    def attend(i, carry):
        for k in range(unroll):
            attend_block(i * unroll + k)
        for k in range(unroll):
            read_swap(i * unroll + k).start()
        return carry

    with jax.named_scope("attend"):
        lax.fori_loop(0, blocks // unroll, attend, 0)

    def out_copy(b):
        at = pl.ds(pl.multiple_of(b * block_len, block_len), block_len)
        return pltpu.make_async_copy(out_rows.at[at], out_ref.at[at], out_sem.at[b])

    def finish(b, carry):
        at = pl.ds(pl.multiple_of(b * block_len, block_len), block_len)
        read_swap(b).wait()
        for j in range(2):
            cols = slice(j * half // 2, (j + 1) * half // 2)
            terms = two_terms(read[at, :], w_out[:, cols], read_far[at, :], w_out_far[:, cols])
            out_rows[at, cols] = (branch[at, cols] + gate[at, cols] * terms).astype(BF16)
        out_copy(b).start()
        return carry

    with jax.named_scope("finish"):
        lax.fori_loop(0, blocks, finish, 0)

    for way in range(2):
        for i, (_, _, need) in enumerate(cuts):
            for d in range(reach - need + 1):
                pl.when((behind[way] >= d) & (beyond[way] >= need))(
                    lambda way=way, d=d, i=i: hop(way, d, i).wait_send()
                )
    for rel in range(1, side):
        for q in range(planes):
            spread_copy(rel, q).wait_send()
    for way in range(2):
        pl.when(behind[way] == 0)(lambda way=way: near_hop(way).wait_send())
    for b in range(blocks):
        out_copy(b).wait()


def mixer(planes, most, block_len, per_block, caps, collective_id, *operands):
    tab, scale, gain, mix, kv, hidden, w_pool, w_query, w_gate, w_branch, w_out = operands
    holders = lax.axis_size("st")
    side = holders // planes
    reach = planes - 1
    tokens, model = hidden.shape
    half = w_gate.shape[1]
    pool_width, width = w_pool.shape[1], w_query.shape[1]
    slot = kv.shape[1:]
    cores = lax.axis_size("tp")
    halo = 2 ** (cores * mix.shape[0])
    nch = len(chunks_of(caps))
    blocks = tokens // block_len
    v = pltpu.VMEM
    dma = pltpu.SemaphoreType.DMA
    flops = 2 * tokens * (model * (pool_width + width + half) + 2 * (pool_width + width) * half)
    return pl.pallas_call(
        functools.partial(mixer_kernel, planes, caps, most, block_len, per_block),
        out_shape=jax.ShapeDtypeStruct((tokens, half), BF16),
        in_specs=[SMEM, SMEM, VMEM, VMEM] + [ANY] * 7,
        out_specs=ANY,
        scratch_shapes=[
            v(kv.shape, BF16),
            v(hidden.shape, BF16),
            v(w_pool.shape, BF16),
            v(w_query.shape, BF16),
            v(w_gate.shape, BF16),
            v((pool_width, half), BF16),
            v((pool_width, half), BF16),
            v((width, half), BF16),
            v((width, half), BF16),
            v((tokens + halo, pool_width), BF16),
            v((tokens, pool_width), BF16),
            v((tokens, pool_width), BF16),
            v((tokens, half), F32),
            v((tokens, half), F32),
            v((tokens, width), BF16),
            v((tokens, width), BF16),
            v((tokens, width), BF16),
            v((2, caps[-1], *slot), BF16),
            *[v((caps[min(reach - d, reach - 2)], *slot), BF16) for _ in range(2) for d in range(1, planes)],
            *[v((caps[0], *slot), BF16) for _ in range(3)],
            v((side - 1, planes * most, *slot), BF16),
            v((holders * most, *slot), BF16),
            v((tokens, half), BF16),
            dma((7,)),
            dma((blocks,)),
            dma((1,)),
            dma((2,)),
            dma((2, reach, nch)),
            dma((2, reach, nch)),
            dma((side - 1, planes)),
            dma((holders,)),
            dma((3 + blocks,)),
            dma((3 + blocks,)),
        ],
        compiler_params=pltpu.CompilerParams(
            collective_id=collective_id, has_side_effects=True, vmem_limit_bytes=LIMIT
        ),
        cost_estimate=pl.CostEstimate(flops=flops, bytes_accessed=32 * 2**20, transcendentals=0),
    )(*operands)


def body(
    planes,
    hidden,
    norm_gain,
    store,
    store_gain,
    passage_ids,
    w_pool,
    pool_mix,
    w_branch,
    w_query,
    w_key,
    w_value,
    sharpness,
    w_out,
    w_gate,
):
    holders = lax.axis_size("st")
    side = holders // planes
    blocks, per_block = passage_ids.shape
    reads = blocks * per_block
    pass_dev = store.shape[0]
    tokens, model = hidden.shape
    most = max(1, 2 * reads // holders)

    one = min(pass_dev, side * most)
    full = tuple(min(pass_dev, k * one) for k in range(1, planes - 1))
    variants = []
    for sixteenths in (9, 10, 11):
        first = one * sixteenths // 16
        lengths = (first, first + pass_dev // 6)
        variants.append(tuple(map(min, lengths, full)))
    variants = (*variants, full)
    tab, own_kv = project(planes, most, variants, passage_ids, store, store_gain, w_key, w_value)
    operands = (
        tab,
        sharpness,
        norm_gain.reshape(1, model),
        pool_mix,
        own_kv,
        hidden,
        w_pool,
        w_query,
        w_gate,
        w_branch,
        w_out,
    )
    run = functools.partial(mixer, planes, most, tokens // blocks, per_block)
    return lax.switch(
        tab[3, 0], [functools.partial(run, caps, i + 1) for i, caps in enumerate(variants)], *operands
    )


def solution(mesh):
    placed = (
        P("st", None),
        P(),
        P("st", None, None),
        P(),
        P("st", None),
        P(None, "tp"),
        P("tp", None, None),
        P("tp", None),
        P(None, "tp"),
        P(None, "tp"),
        P(None, "tp"),
        P("tp"),
        P("tp", None),
        P(None, "tp"),
    )
    return jax.shard_map(
        functools.partial(body, planes_of(mesh)), mesh=mesh, in_specs=placed, out_specs=P("st", "tp"), check_vma=False
    )
```

```python
import functools
import math

import jax
import jax.numpy as jnp
from jax import lax
from jax.experimental import pallas as pl
from jax.experimental.pallas import tpu as pltpu
from jax.sharding import PartitionSpec as P

MESH = pl.DeviceIdType.MESH
F32 = jnp.float32
BF16 = jnp.bfloat16
ANY = pl.BlockSpec(memory_space=pl.ANY)
VMEM = pl.BlockSpec(memory_space=pltpu.VMEM)
SMEM = pl.BlockSpec(memory_space=pltpu.SMEM)


def planes_of(mesh):
    heights = {getattr(d, "coords", (0, 0, 0))[2] for d in mesh.devices.flat}
    return len(heights)


def rms_rows(wide, gain):
    scale = lax.rsqrt(jnp.mean(wide * wide, axis=-1, keepdims=True) + 1e-05)
    return wide * scale * gain


def plan_tables(holders, planes, reads, pass_dev, most, variants, all_ref, tab_ref):
    side = holders // planes
    lanes = 128
    per = lanes // reads
    me = lax.axis_index("st")
    z, c = lax.div(me, side), lax.rem(me, side)

    def lane_of(rows):
        return lax.broadcasted_iota(jnp.int32, (rows, lanes), 1).astype(F32)

    def sub_of(rows, width=lanes):
        return lax.broadcasted_iota(jnp.int32, (rows, width), 0).astype(F32)

    def whole(x, by):
        return jnp.floor((x + 0.5) * (1.0 / by))

    segment = whole(lane_of(1), reads)

    def requests(plane):
        return [requests_row(all_ref, plane, side, per, r, segment) for r in range(side // per)]

    holder_at = lax.broadcasted_iota(jnp.int32, (1, holders), 1).astype(F32)
    plane_at = whole(holder_at, side)
    far_up = jnp.zeros((pass_dev, holders), F32)
    far_down = jnp.zeros((pass_dev, holders), F32)
    near_up = jnp.zeros((pass_dev, holders), F32)
    near_down = jnp.zeros((pass_dev, holders), F32)
    for p in range(planes):
        hits = jnp.zeros((pass_dev, holders), F32)
        for row in requests(p):
            owner = whole(row, pass_dev)
            inside = row - owner * pass_dev
            a = jnp.where(inside == sub_of(pass_dev), 1.0, 0.0).astype(BF16)
            b = jnp.where(owner == sub_of(holders), 1.0, 0.0).astype(BF16)
            hits = hits + lax.dot_general(a, b, (((1,), (1,)), ((), ())), preferred_element_type=F32)
        ahead = jnp.where(hits > 0.5, p - plane_at, 0.0)
        far_up = jnp.maximum(far_up, ahead)
        far_down = jnp.maximum(far_down, -ahead)
        near_up = jnp.where(ahead == 1.0, 1.0, near_up)
        near_down = jnp.where(ahead == -1.0, 1.0, near_down)

    longest = [jnp.zeros((1, holders), F32) for _ in range(planes - 2)]
    for reach, edge in ((near_up, 0), (near_down, planes - 1)):
        count = jnp.sum(reach, axis=0, keepdims=True)
        longest[0] = jnp.maximum(longest[0], jnp.where(plane_at == edge, count, 0.0))
    for reach, left in ((far_up, planes - 1 - plane_at), (far_down, plane_at)):
        for d in range(1, planes):
            count = jnp.sum(jnp.where(reach >= d, 1.0, 0.0), axis=0, keepdims=True)
            for k in range(planes - 2):
                longest[k] = jnp.maximum(longest[k], jnp.where(left - d == k, count, 0.0))
    longest = [jnp.max(x, axis=1, keepdims=True) for x in longest]
    variant = jnp.zeros((1, 1), F32)
    for caps in variants[:-1]:
        over = jnp.zeros((1, 1), F32)
        for k, room in enumerate(caps):
            over = jnp.maximum(over, jnp.where(longest[k] > room, 1.0, 0.0))
        variant = variant + over

    lower = lax.broadcasted_iota(jnp.int32, (pass_dev, pass_dev), 1) < lax.broadcasted_iota(
        jnp.int32, (pass_dev, pass_dev), 0
    )
    diagonal = lax.broadcasted_iota(jnp.int32, (pass_dev, pass_dev), 1) == lax.broadcasted_iota(
        jnp.int32, (pass_dev, pass_dev), 0
    )

    def place_in(reach, q):
        col = jnp.sum(jnp.where(holder_at == (q * side + c).astype(F32), reach, 0.0), axis=1, keepdims=True)
        row = jnp.sum(jnp.where(diagonal, col, 0.0), axis=0, keepdims=True)
        before = (row > col) | ((row == col) & lower)
        return jnp.sum(jnp.where(before, 1.0, 0.0), axis=1, keepdims=True)

    number = sub_of(pass_dev)
    orders = [
        jnp.sum(jnp.where(place_in(reach, z) == lane_of(pass_dev), number, 0.0), axis=0, keepdims=True)
        for reach in (far_up, far_down, jnp.where(z == 0, near_up, near_down))
    ]
    where_at = []
    for q in range(planes):
        reach = jnp.where(q < z, far_up, far_down)
        if q == 0:
            reach = jnp.where(z == 1, near_up, reach)
        if q == planes - 1:
            reach = jnp.where(z == planes - 2, near_down, reach)
        place = place_in(reach, jnp.int32(q))
        where_at.append(jnp.where(q == z, sub_of(pass_dev, 1), place))

    square_sub = sub_of(lanes)
    square_lane = lane_of(lanes)
    close = (square_sub < square_lane) & (whole(square_sub, reads) == whole(square_lane, reads))
    picks = jnp.zeros((planes * most, lanes), F32)
    slots = jnp.zeros((1, lanes), F32)
    for r, row in enumerate(requests(z)):
        owner = whole(row, pass_dev)
        inside = row - owner * pass_dev
        owner_col = jnp.sum(jnp.where(square_sub == square_lane, owner, 0.0), axis=1, keepdims=True)
        rank = jnp.sum(jnp.where(close & (owner_col == owner), 1.0, 0.0), axis=0, keepdims=True)
        of_plane = whole(owner, side)
        of_side = owner - of_plane * side
        here = of_side == c.astype(F32)
        found = jnp.zeros((1, lanes), F32)
        for q in range(planes):
            hit = here & (of_plane == q) & (inside == number)
            found = found + jnp.sum(jnp.where(hit, where_at[q], 0.0), axis=0, keepdims=True)
        target = jnp.where(here, of_plane * most + rank, -1.0)
        values = jnp.where(target == sub_of(planes * most), found, 0.0)
        for t in range(per):
            column = jnp.sum(jnp.where(segment == t, values, 0.0), axis=1, keepdims=True)
            picks = jnp.where(lane_of(planes * most) == r * per + t, column, picks)
        slots = jnp.where(lax.div(c, per) == r, (of_side * planes + of_plane) * most + rank, slots)
    for i, row in enumerate((*orders[:2], slots, variant + jnp.zeros((1, lanes), F32), orders[2])):
        tab_ref[i : i + 1, :] = row.astype(jnp.int32)
    tab_ref[8 : 8 + planes * most, :] = picks.astype(jnp.int32)


def requests_row(all_ref, plane, side, per, r, segment):
    row = jnp.zeros(segment.shape, F32)
    for t in range(per):
        ids = all_ref[plane * side + r * per + t][0:1, :].astype(F32)
        row = jnp.where(segment == t, ids, row)
    return row


def project_kernel(
    holders,
    planes,
    pieces,
    most,
    variants,
    ids_ref,
    store_ref,
    gain_ref,
    wk_hbm,
    wv_hbm,
    tab_ref,
    kv_out,
    kv_ref,
    rows,
    wk_ref,
    wv_ref,
    even,
    odd,
    mine_ids,
    all_ref,
    load_sem,
    send_sem,
    recv_sem,
):
    me = lax.axis_index("st")
    core = lax.axis_index("tp")
    piece = rows.shape[0] // pieces
    width = wk_ref.shape[1]
    pass_dev, length, _ = kv_ref.shape
    passages = piece // length
    per_block, blocks = ids_ref.shape
    reads = blocks * per_block
    weights = [
        pltpu.make_async_copy(src, dst, load_sem.at[pieces + i])
        for i, (src, dst) in enumerate(((wk_hbm, wk_ref), (wv_hbm, wv_ref)))
    ]

    def load(i):
        return pltpu.make_async_copy(
            store_ref.at[pl.ds(i * piece, piece)], rows.at[pl.ds(i * piece, piece)], load_sem.at[i]
        )

    load(0).start()
    for copy in weights:
        copy.start()
    for i in range(1, pieces):
        load(i).start()

    barrier = pltpu.get_barrier_semaphore()

    def other(step):
        return lax.rem(me + step, holders)

    def greet(step, carry):
        pl.semaphore_signal(barrier, inc=1, device_id=(other(step), core), device_id_type=MESH)
        return carry

    lax.fori_loop(1, holders, greet, 0)

    lane = lax.broadcasted_iota(jnp.int32, (per_block, 128), 1).astype(F32)
    lane = lane - reads * jnp.floor((lane + 0.5) * (1.0 / reads))
    block = jnp.floor((lane + 0.5) * (1.0 / per_block))
    inner = lane - block * per_block
    spread_ids = jnp.zeros((per_block, 128), F32)
    for k in range(blocks):
        spread_ids = jnp.where(block == k, ids_ref[:, k : k + 1].astype(F32), spread_ids)
    at_inner = lax.broadcasted_iota(jnp.int32, (per_block, 128), 0).astype(F32) == inner
    row = jnp.sum(jnp.where(at_inner, spread_ids, 0.0), axis=0, keepdims=True)
    mine_ids[...] = jnp.broadcast_to(row, mine_ids.shape).astype(jnp.int32)
    all_ref[me] = jnp.broadcast_to(row, mine_ids.shape).astype(jnp.int32)

    def norm(i, ref):
        load(i).wait()
        start = pl.multiple_of(i * piece, piece)
        ref[...] = rms_rows(rows[pl.ds(start, piece), :].astype(F32), gain_ref[...]).astype(BF16)

    def project(i, ref):
        for half, w_ref in enumerate((wk_ref, wv_ref)):
            part = jnp.dot(ref[...], w_ref[...], preferred_element_type=F32).astype(BF16)
            kv_ref[pl.ds(i * passages, passages), :, half * width : (half + 1) * width] = part.reshape(
                passages, length, width
            )

    with jax.named_scope("kv0"):
        norm(0, even)
        for copy in weights:
            copy.wait()
    with jax.named_scope("greet_all"):
        pl.semaphore_wait(barrier, holders - 1)

    def ids_copy(step):
        return pltpu.make_async_remote_copy(
            src_ref=mine_ids,
            dst_ref=all_ref.at[me],
            send_sem=send_sem.at[0],
            recv_sem=recv_sem.at[0],
            device_id=(other(step), core),
            device_id_type=MESH,
        )

    def send(step, carry):
        ids_copy(step).start()
        return carry

    lax.fori_loop(1, holders, send, 0)

    def leave(i):
        at = pl.ds(i * passages, passages)
        return pltpu.make_async_copy(kv_ref.at[at], kv_out.at[at], load_sem.at[pieces + 2 + i])

    with jax.named_scope("kv1"):
        for i in range(pieces):
            if i + 1 < pieces:
                norm(i + 1, (even, odd)[(i + 1) % 2])
            project(i, (even, odd)[i % 2])
            if i:
                leave(i - 1).start()

    every = all_ref.at[pl.ds(0, holders - 1)]
    with jax.named_scope("ids"):
        pltpu.make_async_remote_copy(
            src_ref=every,
            dst_ref=every,
            send_sem=send_sem.at[0],
            recv_sem=recv_sem.at[0],
            device_id=(other(1), core),
            device_id_type=MESH,
        ).wait()
    with jax.named_scope("tables"):
        leave(pieces - 1).start()
        plan_tables(holders, planes, reads, pass_dev, most, variants, all_ref, tab_ref)
    for i in range(pieces):
        leave(i).wait()


def project(planes, most, variants, ids, store, store_gain, w_key, w_value):
    holders = lax.axis_size("st")
    pass_dev, length, model = store.shape
    pieces = math.gcd(pass_dev, 6)
    width = w_key.shape[1]
    table_rows = 8 + -(-planes * most // 8) * 8
    return pl.pallas_call(
        functools.partial(project_kernel, holders, planes, pieces, most, variants),
        out_shape=(
            jax.ShapeDtypeStruct((table_rows, 128), jnp.int32),
            jax.ShapeDtypeStruct((pass_dev, length, 2 * width), BF16),
        ),
        in_specs=[VMEM, ANY, VMEM, ANY, ANY],
        out_specs=(VMEM, ANY),
        scratch_shapes=[
            pltpu.VMEM((pass_dev, length, 2 * width), BF16),
            pltpu.VMEM((pass_dev * length, model), BF16),
            pltpu.VMEM(w_key.shape, BF16),
            pltpu.VMEM(w_value.shape, BF16),
            pltpu.VMEM((pass_dev * length // pieces, model), BF16),
            pltpu.VMEM((pass_dev * length // pieces, model), BF16),
            pltpu.VMEM((8, 128), jnp.int32),
            pltpu.VMEM((holders, 8, 128), jnp.int32),
            pltpu.SemaphoreType.DMA((2 * pieces + 2,)),
            pltpu.SemaphoreType.DMA((1,)),
            pltpu.SemaphoreType.DMA((1,)),
        ],
        compiler_params=pltpu.CompilerParams(collective_id=0, has_side_effects=True, vmem_limit_bytes=66_000_000),
        cost_estimate=pl.CostEstimate(
            flops=4 * pass_dev * length * model * width, bytes_accessed=store.size * 2, transcendentals=0
        ),
    )(ids.T, store.reshape(pass_dev * length, model), store_gain.reshape(1, model), w_key, w_value)


def chunks_of(caps):
    cut = [(0, caps[0] // 2, 1), (caps[0] // 2, caps[0], 1)]
    for k in range(1, len(caps)):
        if caps[k] > caps[k - 1]:
            cut.append((caps[k - 1], caps[k], k + 1))
    return cut


def mixer_kernel(
    planes,
    caps,
    most,
    block_len,
    per_block,
    tab,
    scale_ref,
    gain_ref,
    mix_ref,
    kv_hbm,
    hidden_hbm,
    w_pool_hbm,
    w_query_hbm,
    w_gate_hbm,
    w_branch_hbm,
    w_out_hbm,
    out_ref,
    kv,
    normed,
    w_pool,
    w_query,
    w_gate,
    w_branch,
    w_branch_far,
    w_out,
    w_out_far,
    pool_in,
    pool_out,
    pool_far,
    branch,
    gate,
    query,
    read,
    read_far,
    own_lists,
    *rest,
):
    reach = planes - 1
    lists = [rest[w * reach : (w + 1) * reach] for w in range(2)]
    near_own, near_up, near_down, picked, final, out_rows, load_sem, out_sem, near_send, near_recv, z_send, z_recv, in_send, in_recv, core_send, core_recv = rest[2 * reach :]
    holders = lax.axis_size("st")
    side = holders // planes
    me = lax.axis_index("st")
    core = lax.axis_index("tp")
    z, c = lax.div(me, side), lax.rem(me, side)
    tokens, model = normed.shape
    half = out_rows.shape[1]
    near = (near_up, near_down)
    cuts = chunks_of(caps)
    beyond = (planes - 1 - z, z)
    behind = (z, planes - 1 - z)
    step_to = (side, -side)

    mine = pl.ds(pl.multiple_of(core * half, half), half)
    theirs = pl.ds(pl.multiple_of((1 - core) * half, half), half)
    loads = [
        pltpu.make_async_copy(src, dst, load_sem.at[i])
        for i, (src, dst) in enumerate(
            (
                (kv_hbm, kv),
                (hidden_hbm, normed),
                (w_pool_hbm, w_pool),
                (w_query_hbm, w_query),
                (w_branch_hbm.at[:, mine], w_branch),
                (w_gate_hbm, w_gate),
                (w_out_hbm.at[:, mine], w_out),
            )
        )
    ]
    for copy in loads:
        copy.start()

    barrier = pltpu.get_barrier_semaphore()

    def greet(device):
        pl.semaphore_signal(barrier, inc=1, device_id=device, device_id_type=MESH)

    def mate_of(k):
        mate = c
        for b in range(k.bit_length()):
            if k >> b & 1:
                mate = mate + (1 << b) * (1 - 2 * lax.rem(lax.div(c, 1 << b), 2))
        return mate

    for k in range(1, side):
        greet((z * side + mate_of(k), core))
    greet((me, 1 - core))
    for way in range(2):
        pl.when(beyond[way] >= 1)(lambda way=way: greet((me + step_to[way], core)))

    def partner(src, dst, i):
        return pltpu.make_async_remote_copy(
            src_ref=src,
            dst_ref=dst,
            send_sem=core_send.at[i],
            recv_sem=core_recv.at[i],
            device_id=(me, 1 - core),
            device_id_type=MESH,
        )

    weight_swaps = [
        partner(w_branch_hbm.at[:, theirs], w_branch_far, 0),
        partner(w_out_hbm.at[:, theirs], w_out_far, 1),
    ]
    pool_swap = partner(pool_out, pool_far, 2)

    def hop(way, d, i):
        first, last, _ = cuts[i]
        src = own_lists.at[way] if d == 0 else lists[way][d - 1]
        return pltpu.make_async_remote_copy(
            src_ref=src.at[pl.ds(first, last - first)],
            dst_ref=lists[way][d].at[pl.ds(first, last - first)],
            send_sem=z_send.at[way, d, i],
            recv_sem=z_recv.at[way, d, i],
            device_id=(me + step_to[way], core),
            device_id_type=MESH,
        )

    def arrive(way, d, i):
        first, last, _ = cuts[i]
        ref = lists[way][d - 1].at[pl.ds(first, last - first)]
        pltpu.make_async_remote_copy(
            src_ref=ref,
            dst_ref=ref,
            send_sem=z_send.at[way, d - 1, i],
            recv_sem=z_recv.at[way, d - 1, i],
            device_id=(me, 1 - core),
            device_id_type=MESH,
        ).wait_recv()

    def near_hop(way):
        return pltpu.make_async_remote_copy(
            src_ref=near_own,
            dst_ref=near[way],
            send_sem=near_send.at[0],
            recv_sem=near_recv.at[way],
            device_id=(me + step_to[way], core),
            device_id_type=MESH,
        )

    def near_arrive(way):
        pltpu.make_async_remote_copy(
            src_ref=near[way],
            dst_ref=near[way],
            send_sem=near_send.at[0],
            recv_sem=near_recv.at[way],
            device_id=(me, 1 - core),
            device_id_type=MESH,
        ).wait_recv()

    def forward(d, i, here):
        need = cuts[i][2]
        if need > reach - d:
            return
        for way in range(2):

            def go(way=way):
                arrive(way, d, i)
                hop(way, d, i).start()

            pl.when(here(way) & (behind[way] >= d) & (beyond[way] >= need))(go)

    def keep(d, here):
        for i, (_, _, need) in enumerate(cuts):
            if need > reach - d + 1:
                continue
            for way in range(2):
                pl.when(here(way) & (behind[way] >= d) & (beyond[way] + 1 == need))(lambda way=way, i=i: arrive(way, d, i))


    def spread_copy(rel, q):
        mate = z * side + mate_of(rel)
        return pltpu.make_async_remote_copy(
            src_ref=picked.at[rel - 1, pl.ds(q * most, most)],
            dst_ref=final.at[pl.ds((c * planes + q) * most, most)],
            send_sem=in_send.at[rel - 1, q],
            recv_sem=in_recv.at[c * planes + q],
            device_id=(mate, core),
            device_id_type=MESH,
        )

    mates = list(range(side - 1, 0, -1))

    def pick(src, q, k):
        for j in range(most):
            slot = src[tab[8 + q * most + j, mate_of(k) if k else c]]
            if k:
                picked[k - 1, q * most + j] = slot
            else:
                final[(c * planes + q) * most + j] = slot

    def spread(src, q):
        for n, k in enumerate((*mates, 0)):
            pick(src, q, k)
            if n:
                spread_copy(mates[n - 1], q).start()

    def spread_from(d, here):
        for way in range(2):
            q = z - d if way == 0 else z + d
            pl.when(here(way) & (behind[way] >= d))(lambda way=way, q=q: spread(lists[way][d - 1], q))

    def spread_near():
        for way in range(2):

            def go(way=way):
                near_arrive(way)
                spread(near[way], z - 1 if way == 0 else z + 1)

            pl.when((behind[way] == 1) & (beyond[way] >= 1))(go)

    with jax.named_scope("build"):
        loads[0].wait()
        for way in range(2):
            for s in range(caps[-1]):
                own_lists[way, s] = kv[tab[way, s]]
        for s in range(caps[0]):
            near_own[s] = kv[tab[4, s]]
        for k in range(side):
            pick(kv, z, k)
    with jax.named_scope("greet"):
        pl.semaphore_wait(barrier, side + (z + reach - 1) // reach + (beyond[0] + reach - 1) // reach)
    with jax.named_scope("first_sends"):
        for way in range(2):
            pl.when(behind[way] == 0)(lambda way=way: near_hop(way).start())
        for i, (_, _, need) in enumerate(cuts):
            for way in range(2):
                pl.when(beyond[way] >= need)(lambda way=way, i=i: hop(way, 0, i).start())
        for k in mates:
            spread_copy(k, z).start()
        for copy in weight_swaps:
            copy.start()

    def norm(lo, hi, rows=32):
        def body(i, carry):
            at = pl.ds(pl.multiple_of(i * rows, rows), rows)
            normed[at, :] = rms_rows(normed[at, :].astype(F32), gain_ref[...]).astype(BF16)
            return carry

        lax.fori_loop(lo // rows, hi // rows, body, 0)

    piece = math.gcd(tokens, 256)
    pieces = tokens // piece
    halo = pool_in.shape[0] - tokens
    groups, group_dim = mix_ref.shape[:2]

    def project_rows(lo, hi):
        def body(i, carry):
            at = pl.ds(pl.multiple_of(i * piece, piece), piece)
            rows = normed[at, :]
            pool_in[pl.ds(pl.multiple_of(halo + i * piece, halo), piece), :] = jnp.dot(
                rows, w_pool[...], preferred_element_type=F32
            ).astype(BF16)
            query[at, :] = jnp.dot(rows, w_query[...], preferred_element_type=F32).astype(BF16)
            return carry

        lax.fori_loop(lo, hi, body, 0)

    def pool_rows(i, carry):
        at = pl.ds(pl.multiple_of(i * piece, piece), piece)
        position = i * piece + lax.broadcasted_iota(jnp.int32, (piece, 1), 0)
        for g in range(groups):
            cols = slice(g * group_dim, (g + 1) * group_dim)
            wide = pool_in[pl.ds(pl.multiple_of(i * piece, piece), piece + halo), cols].astype(F32)
            sums = []
            total = wide
            shift = 1
            while shift < halo:
                total = total + pltpu.roll(total, shift, 0)
                sums.append(total[halo:])
                shift *= 2
            per_core = [sums[k * groups + g] for k in range(len(sums) // groups)]
            level = per_core[0]
            window = 2 ** (g + 1)
            for k in range(1, len(per_core)):
                level = jnp.where(core == k, per_core[k], level)
                window = jnp.where(core == k, 2 ** (k * groups + g + 1), window)
            count = jnp.minimum(position + 1, window).astype(F32)
            pooled = (level / count - wide[halo:]).astype(BF16)
            pool_out[at, cols] = jnp.dot(pooled, mix_ref[g], preferred_element_type=F32).astype(BF16)
        return carry

    def gate_rows(lo, hi):
        def body(i, carry):
            at = pl.ds(pl.multiple_of(i * piece, piece), piece)
            for j in range(2):
                cols = slice(j * half // 2, (j + 1) * half // 2)
                logits = jnp.dot(normed[at, :], w_gate[:, cols], preferred_element_type=F32)
                gate[at, cols] = 1.0 / (1.0 + jnp.exp(-logits))
            return carry

        lax.fori_loop(lo, hi, body, 0)

    def two_terms(a, w, a_far, w_far):
        near = jnp.dot(a, w, preferred_element_type=F32).astype(BF16).astype(F32)
        far = jnp.dot(a_far, w_far, preferred_element_type=F32).astype(BF16).astype(F32)
        return near + far

    def branch_rows(i, carry):
        at = pl.ds(pl.multiple_of(i * piece, piece), piece)
        for j in range(2):
            cols = slice(j * half // 2, (j + 1) * half // 2)
            branch[at, cols] = two_terms(
                pool_out[at, :], w_branch[:, cols], pool_far[at, :], w_branch_far[:, cols]
            )
        return carry

    def at_edge(way):
        return beyond[way] == 0

    def inside(way):
        return beyond[way] >= 1

    def from_edge(way):
        return behind[way] == 1

    def from_inside(way):
        return behind[way] >= 2

    with jax.named_scope("norm"):
        loads[1].wait()
        norm(0, tokens)
    with jax.named_scope("project"):
        loads[2].wait()
        loads[3].wait()
        pool_in[:halo, :] = jnp.zeros((halo, pool_in.shape[1]), BF16)
        project_rows(0, pieces)
    with jax.named_scope("pool"):
        lax.fori_loop(0, pieces, pool_rows, 0)
        pool_swap.start()
    with jax.named_scope("step0"):
        forward(1, 0, from_inside)
    with jax.named_scope("gate"):
        loads[5].wait()
        gate_rows(0, pieces // 2)
    with jax.named_scope("step1"):
        forward(1, 1, from_inside)
        keep(1, at_edge)
        spread_from(1, at_edge)
        spread_near()
    with jax.named_scope("gate"):
        gate_rows(pieces // 2, pieces)
    with jax.named_scope("branch"):
        loads[4].wait()
        loads[6].wait()
        for copy in weight_swaps:
            copy.wait()
        pool_swap.wait()
        lax.fori_loop(0, pieces, branch_rows, 0)
    with jax.named_scope("step2"):
        for i in range(2, len(cuts)):
            forward(1, i, from_inside)
        keep(1, inside)
        spread_from(1, lambda way: inside(way) & from_inside(way))
        forward(1, 0, from_edge)
    for d in range(2, planes):
        with jax.named_scope(f"step{d + 1}"):
            forward(d, 0, inside)
            keep(d, at_edge)
            spread_from(d, at_edge)
            if d == 2:
                for i in range(1, len(cuts)):
                    forward(1, i, from_edge)
            for i in range(1, len(cuts)):
                forward(d, i, inside)
            keep(d, inside)
            spread_from(d, inside)

    with jax.named_scope("arrivals"):
        for rel in range(1, side):
            source = mate_of(rel)
            for q in range(planes):
                at = pl.ds((source * planes + q) * most, most)
                pltpu.make_async_remote_copy(
                    src_ref=final.at[at],
                    dst_ref=final.at[at],
                    send_sem=in_send.at[rel - 1, q],
                    recv_sem=in_recv.at[source * planes + q],
                    device_id=(me, 1 - core),
                    device_id_type=MESH,
                ).wait_recv()

    blocks = tokens // block_len
    heads = scale_ref.shape[0]
    width = query.shape[1]
    head_dim = width // heads
    reads = blocks * per_block
    slot_base = lax.rem(c, 128 // reads) * reads

    def read_swap(b):
        at = pl.ds(pl.multiple_of(b * block_len, block_len), block_len)
        return partner(read.at[at], read_far.at[at], 3 + b)

    def attend_block(b):
        at = pl.ds(pl.multiple_of(b * block_len, block_len), block_len)
        memory = jnp.concatenate(
            [final[tab[2, slot_base + b * per_block + i]] for i in range(per_block)], axis=0
        )
        for h in range(heads):
            cut = slice(h * head_dim, (h + 1) * head_dim)
            scale = scale_ref[h] * (1.0 / math.sqrt(head_dim))
            scores = lax.dot_general(
                query[at, cut], memory[:, cut], (((1,), (1,)), ((), ())), preferred_element_type=F32
            )
            scores = scores * scale
            top = jnp.exp(scores - jnp.max(scores, axis=-1, keepdims=True))
            weights = (top * (1.0 / jnp.sum(top, axis=-1, keepdims=True))).astype(BF16)
            read[at, cut] = jnp.dot(
                weights, memory[:, width + h * head_dim : width + (h + 1) * head_dim], preferred_element_type=F32
            ).astype(BF16)

    unroll = math.gcd(blocks, 4)

    def attend(i, carry):
        for k in range(unroll):
            attend_block(i * unroll + k)
        for k in range(unroll):
            read_swap(i * unroll + k).start()
        return carry

    with jax.named_scope("attend"):
        lax.fori_loop(0, blocks // unroll, attend, 0)

    joint = math.gcd(blocks, 2)

    def out_copy(i):
        at = pl.ds(pl.multiple_of(i * joint * block_len, block_len), joint * block_len)
        return pltpu.make_async_copy(out_rows.at[at], out_ref.at[at], out_sem.at[i])

    def finish(i, carry):
        at = pl.ds(pl.multiple_of(i * joint * block_len, block_len), joint * block_len)
        for k in range(joint):
            read_swap(i * joint + k).wait()
        for j in range(2):
            cols = slice(j * half // 2, (j + 1) * half // 2)
            terms = two_terms(read[at, :], w_out[:, cols], read_far[at, :], w_out_far[:, cols])
            out_rows[at, cols] = (branch[at, cols] + gate[at, cols] * terms).astype(BF16)
        out_copy(i).start()
        return carry

    with jax.named_scope("finish"):
        lax.fori_loop(0, blocks // joint, finish, 0)

    for way in range(2):
        for i, (_, _, need) in enumerate(cuts):
            for d in range(reach - need + 1):
                pl.when((behind[way] >= d) & (beyond[way] >= need))(
                    lambda way=way, d=d, i=i: hop(way, d, i).wait_send()
                )
    for rel in range(1, side):
        for q in range(planes):
            spread_copy(rel, q).wait_send()
    for way in range(2):
        pl.when(behind[way] == 0)(lambda way=way: near_hop(way).wait_send())
    for i in range(blocks // joint):
        out_copy(i).wait()


def mixer(planes, most, block_len, per_block, caps, collective_id, *operands):
    tab, scale, gain, mix, kv, hidden, w_pool, w_query, w_gate, w_branch, w_out = operands
    holders = lax.axis_size("st")
    side = holders // planes
    reach = planes - 1
    tokens, model = hidden.shape
    half = w_gate.shape[1]
    pool_width, width = w_pool.shape[1], w_query.shape[1]
    slot = kv.shape[1:]
    cores = lax.axis_size("tp")
    halo = 2 ** (cores * mix.shape[0])
    nch = len(chunks_of(caps))
    blocks = tokens // block_len
    v = pltpu.VMEM
    dma = pltpu.SemaphoreType.DMA
    flops = 2 * tokens * (model * (pool_width + width + half) + 2 * (pool_width + width) * half)
    return pl.pallas_call(
        functools.partial(mixer_kernel, planes, caps, most, block_len, per_block),
        out_shape=jax.ShapeDtypeStruct((tokens, half), BF16),
        in_specs=[SMEM, SMEM, VMEM, VMEM] + [ANY] * 7,
        out_specs=ANY,
        scratch_shapes=[
            v(kv.shape, BF16),
            v(hidden.shape, BF16),
            v(w_pool.shape, BF16),
            v(w_query.shape, BF16),
            v(w_gate.shape, BF16),
            v((pool_width, half), BF16),
            v((pool_width, half), BF16),
            v((width, half), BF16),
            v((width, half), BF16),
            v((tokens + halo, pool_width), BF16),
            v((tokens, pool_width), BF16),
            v((tokens, pool_width), BF16),
            v((tokens, half), F32),
            v((tokens, half), F32),
            v((tokens, width), BF16),
            v((tokens, width), BF16),
            v((tokens, width), BF16),
            v((2, caps[-1], *slot), BF16),
            *[v((caps[min(reach - d, reach - 2)], *slot), BF16) for _ in range(2) for d in range(1, planes)],
            *[v((caps[0], *slot), BF16) for _ in range(3)],
            v((side - 1, planes * most, *slot), BF16),
            v((holders * most, *slot), BF16),
            v((tokens, half), BF16),
            dma((7,)),
            dma((blocks,)),
            dma((1,)),
            dma((2,)),
            dma((2, reach, nch)),
            dma((2, reach, nch)),
            dma((side - 1, planes)),
            dma((holders,)),
            dma((3 + blocks,)),
            dma((3 + blocks,)),
        ],
        compiler_params=pltpu.CompilerParams(
            collective_id=collective_id, has_side_effects=True, vmem_limit_bytes=55 * 2**20
        ),
        cost_estimate=pl.CostEstimate(flops=flops, bytes_accessed=32 * 2**20, transcendentals=0),
    )(*operands)


def body(
    planes,
    hidden,
    norm_gain,
    store,
    store_gain,
    passage_ids,
    w_pool,
    pool_mix,
    w_branch,
    w_query,
    w_key,
    w_value,
    sharpness,
    w_out,
    w_gate,
):
    holders = lax.axis_size("st")
    side = holders // planes
    blocks, per_block = passage_ids.shape
    reads = blocks * per_block
    pass_dev = store.shape[0]
    tokens, model = hidden.shape
    most = max(1, 2 * reads // holders)

    one = min(pass_dev, side * most)
    full = tuple(min(pass_dev, k * one) for k in range(1, planes - 1))
    variants = []
    for sixteenths in (9, 10, 11):
        first = one * sixteenths // 16
        lengths = (first, first + pass_dev // 6)
        variants.append(tuple(map(min, lengths, full)))
    variants = (*variants, full)
    tab, own_kv = project(planes, most, variants, passage_ids, store, store_gain, w_key, w_value)
    operands = (
        tab,
        sharpness,
        norm_gain.reshape(1, model),
        pool_mix,
        own_kv,
        hidden,
        w_pool,
        w_query,
        w_gate,
        w_branch,
        w_out,
    )
    run = functools.partial(mixer, planes, most, tokens // blocks, per_block)
    return lax.switch(
        tab[3, 0], [functools.partial(run, caps, i + 1) for i, caps in enumerate(variants)], *operands
    )


def solution(mesh):
    placed = (
        P("st", None),
        P(),
        P("st", None, None),
        P(),
        P("st", None),
        P(None, "tp"),
        P("tp", None, None),
        P("tp", None),
        P(None, "tp"),
        P(None, "tp"),
        P(None, "tp"),
        P("tp"),
        P("tp", None),
        P(None, "tp"),
    )
    return jax.shard_map(
        functools.partial(body, planes_of(mesh)), mesh=mesh, in_specs=placed, out_specs=P("st", "tp"), check_vma=False
    )
```

```python
import functools
import math

import jax
import jax.numpy as jnp
from jax import lax
from jax.experimental import pallas as pl
from jax.experimental.pallas import tpu as pltpu
from jax.sharding import PartitionSpec as P

MESH = pl.DeviceIdType.MESH
F32 = jnp.float32
BF16 = jnp.bfloat16
ANY = pl.BlockSpec(memory_space=pl.ANY)
VMEM = pl.BlockSpec(memory_space=pltpu.VMEM)
PIN = pl.BlockSpec(memory_space=pltpu.HBM)
SMEM = pl.BlockSpec(memory_space=pltpu.SMEM)


def planes_of(mesh):
    heights = {getattr(d, "coords", (0, 0, 0))[2] for d in mesh.devices.flat}
    return len(heights)


def rms_rows(wide, gain):
    scale = lax.rsqrt(jnp.mean(wide * wide, axis=-1, keepdims=True) + 1e-05)
    return wide * scale * gain


def plan_tables(holders, planes, reads, pass_dev, most, variants, all_ref, tab_ref):
    side = holders // planes
    lanes = 128
    per = lanes // reads
    me = lax.axis_index("st")
    z, c = lax.div(me, side), lax.rem(me, side)

    def lane_of(rows):
        return lax.broadcasted_iota(jnp.int32, (rows, lanes), 1).astype(F32)

    def sub_of(rows, width=lanes):
        return lax.broadcasted_iota(jnp.int32, (rows, width), 0).astype(F32)

    def whole(x, by):
        return jnp.floor((x + 0.5) * (1.0 / by))

    segment = whole(lane_of(1), reads)

    def requests(plane):
        return [requests_row(all_ref, plane, side, per, r, segment) for r in range(side // per)]

    holder_at = lax.broadcasted_iota(jnp.int32, (1, holders), 1).astype(F32)
    plane_at = whole(holder_at, side)
    far_up = jnp.zeros((pass_dev, holders), F32)
    far_down = jnp.zeros((pass_dev, holders), F32)
    near_up = jnp.zeros((pass_dev, holders), F32)
    near_down = jnp.zeros((pass_dev, holders), F32)
    for p in range(planes):
        hits = jnp.zeros((pass_dev, holders), F32)
        for row in requests(p):
            owner = whole(row, pass_dev)
            inside = row - owner * pass_dev
            a = jnp.where(inside == sub_of(pass_dev), 1.0, 0.0).astype(BF16)
            b = jnp.where(owner == sub_of(holders), 1.0, 0.0).astype(BF16)
            hits = hits + lax.dot_general(a, b, (((1,), (1,)), ((), ())), preferred_element_type=F32)
        ahead = jnp.where(hits > 0.5, p - plane_at, 0.0)
        far_up = jnp.maximum(far_up, ahead)
        far_down = jnp.maximum(far_down, -ahead)
        near_up = jnp.where(ahead == 1.0, 1.0, near_up)
        near_down = jnp.where(ahead == -1.0, 1.0, near_down)

    longest = [jnp.zeros((1, holders), F32) for _ in range(planes - 2)]
    for reach, edge in ((near_up, 0), (near_down, planes - 1)):
        count = jnp.sum(reach, axis=0, keepdims=True)
        longest[0] = jnp.maximum(longest[0], jnp.where(plane_at == edge, count, 0.0))
    for reach, left in ((far_up, planes - 1 - plane_at), (far_down, plane_at)):
        for d in range(1, planes):
            count = jnp.sum(jnp.where(reach >= d, 1.0, 0.0), axis=0, keepdims=True)
            for k in range(planes - 2):
                longest[k] = jnp.maximum(longest[k], jnp.where(left - d == k, count, 0.0))
    longest = [jnp.max(x, axis=1, keepdims=True) for x in longest]
    variant = jnp.zeros((1, 1), F32)
    for caps in variants[:-1]:
        over = jnp.zeros((1, 1), F32)
        for k, room in enumerate(caps):
            over = jnp.maximum(over, jnp.where(longest[k] > room, 1.0, 0.0))
        variant = variant + over

    lower = lax.broadcasted_iota(jnp.int32, (pass_dev, pass_dev), 1) < lax.broadcasted_iota(
        jnp.int32, (pass_dev, pass_dev), 0
    )
    diagonal = lax.broadcasted_iota(jnp.int32, (pass_dev, pass_dev), 1) == lax.broadcasted_iota(
        jnp.int32, (pass_dev, pass_dev), 0
    )

    def place_in(reach, q):
        col = jnp.sum(jnp.where(holder_at == (q * side + c).astype(F32), reach, 0.0), axis=1, keepdims=True)
        row = jnp.sum(jnp.where(diagonal, col, 0.0), axis=0, keepdims=True)
        before = (row > col) | ((row == col) & lower)
        return jnp.sum(jnp.where(before, 1.0, 0.0), axis=1, keepdims=True)

    number = sub_of(pass_dev)
    orders = [
        jnp.sum(jnp.where(place_in(reach, z) == lane_of(pass_dev), number, 0.0), axis=0, keepdims=True)
        for reach in (far_up, far_down, jnp.where(z == 0, near_up, near_down))
    ]
    where_at = []
    for q in range(planes):
        reach = jnp.where(q < z, far_up, far_down)
        if q == 0:
            reach = jnp.where(z == 1, near_up, reach)
        if q == planes - 1:
            reach = jnp.where(z == planes - 2, near_down, reach)
        place = place_in(reach, jnp.int32(q))
        where_at.append(jnp.where(q == z, sub_of(pass_dev, 1), place))

    square_sub = sub_of(lanes)
    square_lane = lane_of(lanes)
    close = (square_sub < square_lane) & (whole(square_sub, reads) == whole(square_lane, reads))
    picks = jnp.zeros((planes * most, lanes), F32)
    slots = jnp.zeros((1, lanes), F32)
    for r, row in enumerate(requests(z)):
        owner = whole(row, pass_dev)
        inside = row - owner * pass_dev
        owner_col = jnp.sum(jnp.where(square_sub == square_lane, owner, 0.0), axis=1, keepdims=True)
        rank = jnp.sum(jnp.where(close & (owner_col == owner), 1.0, 0.0), axis=0, keepdims=True)
        of_plane = whole(owner, side)
        of_side = owner - of_plane * side
        here = of_side == c.astype(F32)
        found = jnp.zeros((1, lanes), F32)
        for q in range(planes):
            hit = here & (of_plane == q) & (inside == number)
            found = found + jnp.sum(jnp.where(hit, where_at[q], 0.0), axis=0, keepdims=True)
        target = jnp.where(here, of_plane * most + rank, -1.0)
        values = jnp.where(target == sub_of(planes * most), found, 0.0)
        for t in range(per):
            column = jnp.sum(jnp.where(segment == t, values, 0.0), axis=1, keepdims=True)
            picks = jnp.where(lane_of(planes * most) == r * per + t, column, picks)
        slots = jnp.where(lax.div(c, per) == r, (of_side * planes + of_plane) * most + rank, slots)
    for i, row in enumerate((*orders[:2], slots, variant + jnp.zeros((1, lanes), F32), orders[2])):
        tab_ref[i : i + 1, :] = row.astype(jnp.int32)
    tab_ref[8 : 8 + planes * most, :] = picks.astype(jnp.int32)


def requests_row(all_ref, plane, side, per, r, segment):
    row = jnp.zeros(segment.shape, F32)
    for t in range(per):
        ids = all_ref[plane * side + r * per + t][0:1, :].astype(F32)
        row = jnp.where(segment == t, ids, row)
    return row


def project_kernel(
    holders,
    planes,
    pieces,
    most,
    variants,
    ids_ref,
    store_ref,
    gain_ref,
    wk_hbm,
    wv_hbm,
    tab_ref,
    kv_ref,
    rows,
    wk_ref,
    wv_ref,
    even,
    odd,
    mine_ids,
    all_ref,
    load_sem,
    send_sem,
    recv_sem,
):
    me = lax.axis_index("st")
    core = lax.axis_index("tp")
    piece = rows.shape[0] // pieces
    width = wk_ref.shape[1]
    pass_dev, length, _ = kv_ref.shape
    passages = piece // length
    per_block, blocks = ids_ref.shape
    reads = blocks * per_block
    weights = [
        pltpu.make_async_copy(src, dst, load_sem.at[pieces + i])
        for i, (src, dst) in enumerate(((wk_hbm, wk_ref), (wv_hbm, wv_ref)))
    ]

    def load(i):
        return pltpu.make_async_copy(
            store_ref.at[pl.ds(i * piece, piece)], rows.at[pl.ds(i * piece, piece)], load_sem.at[i]
        )

    load(0).start()
    for copy in weights:
        copy.start()
    for i in range(1, pieces):
        load(i).start()

    barrier = pltpu.get_barrier_semaphore()

    def other(step):
        return lax.rem(me + step, holders)

    def greet(step, carry):
        pl.semaphore_signal(barrier, inc=1, device_id=(other(step), core), device_id_type=MESH)
        return carry

    lax.fori_loop(1, holders, greet, 0)

    lane = lax.broadcasted_iota(jnp.int32, (per_block, 128), 1).astype(F32)
    lane = lane - reads * jnp.floor((lane + 0.5) * (1.0 / reads))
    block = jnp.floor((lane + 0.5) * (1.0 / per_block))
    inner = lane - block * per_block
    spread_ids = jnp.zeros((per_block, 128), F32)
    for k in range(blocks):
        spread_ids = jnp.where(block == k, ids_ref[:, k : k + 1].astype(F32), spread_ids)
    at_inner = lax.broadcasted_iota(jnp.int32, (per_block, 128), 0).astype(F32) == inner
    row = jnp.sum(jnp.where(at_inner, spread_ids, 0.0), axis=0, keepdims=True)
    mine_ids[...] = jnp.broadcast_to(row, mine_ids.shape).astype(jnp.int32)
    all_ref[me] = jnp.broadcast_to(row, mine_ids.shape).astype(jnp.int32)

    def norm(i, ref):
        load(i).wait()
        start = pl.multiple_of(i * piece, piece)
        ref[...] = rms_rows(rows[pl.ds(start, piece), :].astype(F32), gain_ref[...]).astype(BF16)

    def project(i, ref):
        for half, w_ref in enumerate((wk_ref, wv_ref)):
            part = jnp.dot(ref[...], w_ref[...], preferred_element_type=F32).astype(BF16)
            kv_ref[pl.ds(i * passages, passages), :, half * width : (half + 1) * width] = part.reshape(
                passages, length, width
            )

    with jax.named_scope("kv0"):
        norm(0, even)
        for copy in weights:
            copy.wait()
    with jax.named_scope("greet_all"):
        pl.semaphore_wait(barrier, holders - 1)

    def ids_copy(step):
        return pltpu.make_async_remote_copy(
            src_ref=mine_ids,
            dst_ref=all_ref.at[me],
            send_sem=send_sem.at[0],
            recv_sem=recv_sem.at[0],
            device_id=(other(step), core),
            device_id_type=MESH,
        )

    def send(step, carry):
        ids_copy(step).start()
        return carry

    lax.fori_loop(1, holders, send, 0)

    with jax.named_scope("kv1"):
        for i in range(pieces):
            if i + 1 < pieces:
                norm(i + 1, (even, odd)[(i + 1) % 2])
            project(i, (even, odd)[i % 2])

    every = all_ref.at[pl.ds(0, holders - 1)]
    with jax.named_scope("ids"):
        pltpu.make_async_remote_copy(
            src_ref=every,
            dst_ref=every,
            send_sem=send_sem.at[0],
            recv_sem=recv_sem.at[0],
            device_id=(other(1), core),
            device_id_type=MESH,
        ).wait()
    with jax.named_scope("tables"):
        plan_tables(holders, planes, reads, pass_dev, most, variants, all_ref, tab_ref)


def project(planes, most, variants, ids, store, store_gain, w_key, w_value):
    holders = lax.axis_size("st")
    pass_dev, length, model = store.shape
    pieces = math.gcd(pass_dev, 6)
    width = w_key.shape[1]
    table_rows = 8 + -(-planes * most // 8) * 8
    return pl.pallas_call(
        functools.partial(project_kernel, holders, planes, pieces, most, variants),
        out_shape=(
            jax.ShapeDtypeStruct((table_rows, 128), jnp.int32),
            pltpu.VMEM((pass_dev, length, 2 * width), BF16),
        ),
        in_specs=[VMEM, PIN, VMEM, PIN, PIN],
        out_specs=(VMEM, VMEM),
        scratch_shapes=[
            pltpu.VMEM((pass_dev * length, model), BF16),
            pltpu.VMEM(w_key.shape, BF16),
            pltpu.VMEM(w_value.shape, BF16),
            pltpu.VMEM((pass_dev * length // pieces, model), BF16),
            pltpu.VMEM((pass_dev * length // pieces, model), BF16),
            pltpu.VMEM((8, 128), jnp.int32),
            pltpu.VMEM((holders, 8, 128), jnp.int32),
            pltpu.SemaphoreType.DMA((2 * pieces + 2,)),
            pltpu.SemaphoreType.DMA((1,)),
            pltpu.SemaphoreType.DMA((1,)),
        ],
        compiler_params=pltpu.CompilerParams(collective_id=0, has_side_effects=True, vmem_limit_bytes=65_250_000),
        cost_estimate=pl.CostEstimate(
            flops=4 * pass_dev * length * model * width, bytes_accessed=store.size * 2, transcendentals=0
        ),
    )(ids.T, store.reshape(pass_dev * length, model), store_gain.reshape(1, model), w_key, w_value)


def chunks_of(caps):
    cut = [(0, caps[0] // 2, 1), (caps[0] // 2, caps[0], 1)]
    for k in range(1, len(caps)):
        if caps[k] > caps[k - 1]:
            cut.append((caps[k - 1], caps[k], k + 1))
    return cut


def mixer_kernel(
    planes,
    caps,
    most,
    block_len,
    per_block,
    tab,
    scale_ref,
    gain_ref,
    mix_ref,
    kv,
    hidden_hbm,
    w_pool_hbm,
    w_query_hbm,
    w_gate_hbm,
    w_branch_hbm,
    w_out_hbm,
    out_ref,
    normed,
    w_pool,
    w_query,
    w_gate,
    w_branch,
    w_branch_far,
    w_out,
    w_out_far,
    pool_in,
    pool_out,
    pool_far,
    branch,
    gate,
    query,
    read,
    read_far,
    own_lists,
    *rest,
):
    reach = planes - 1
    lists = [rest[w * reach : (w + 1) * reach] for w in range(2)]
    near_own, near_up, near_down, picked, final, out_rows, load_sem, out_sem, near_send, near_recv, z_send, z_recv, in_send, in_recv, core_send, core_recv = rest[2 * reach :]
    holders = lax.axis_size("st")
    side = holders // planes
    me = lax.axis_index("st")
    core = lax.axis_index("tp")
    z, c = lax.div(me, side), lax.rem(me, side)
    tokens, model = normed.shape
    half = out_rows.shape[1]
    near = (near_up, near_down)
    cuts = chunks_of(caps)
    beyond = (planes - 1 - z, z)
    behind = (z, planes - 1 - z)
    step_to = (side, -side)

    mine = pl.ds(pl.multiple_of(core * half, half), half)
    theirs = pl.ds(pl.multiple_of((1 - core) * half, half), half)
    loads = [
        pltpu.make_async_copy(src, dst, load_sem.at[i])
        for i, (src, dst) in enumerate(
            (
                (hidden_hbm, normed),
                (w_pool_hbm, w_pool),
                (w_query_hbm, w_query),
                (w_branch_hbm.at[:, mine], w_branch),
                (w_gate_hbm, w_gate),
                (w_out_hbm.at[:, mine], w_out),
            )
        )
    ]
    for copy in loads:
        copy.start()

    barrier = pltpu.get_barrier_semaphore()

    def greet(device):
        pl.semaphore_signal(barrier, inc=1, device_id=device, device_id_type=MESH)

    def mate_of(k):
        mate = c
        for b in range(k.bit_length()):
            if k >> b & 1:
                mate = mate + (1 << b) * (1 - 2 * lax.rem(lax.div(c, 1 << b), 2))
        return mate

    for k in range(1, side):
        greet((z * side + mate_of(k), core))
    greet((me, 1 - core))
    for way in range(2):
        pl.when(beyond[way] >= 1)(lambda way=way: greet((me + step_to[way], core)))

    def partner(src, dst, i):
        return pltpu.make_async_remote_copy(
            src_ref=src,
            dst_ref=dst,
            send_sem=core_send.at[i],
            recv_sem=core_recv.at[i],
            device_id=(me, 1 - core),
            device_id_type=MESH,
        )

    weight_swaps = [
        partner(w_branch_hbm.at[:, theirs], w_branch_far, 0),
        partner(w_out_hbm.at[:, theirs], w_out_far, 1),
    ]
    pool_swap = partner(pool_out, pool_far, 2)

    def hop(way, d, i):
        first, last, _ = cuts[i]
        src = own_lists.at[way] if d == 0 else lists[way][d - 1]
        return pltpu.make_async_remote_copy(
            src_ref=src.at[pl.ds(first, last - first)],
            dst_ref=lists[way][d].at[pl.ds(first, last - first)],
            send_sem=z_send.at[way, d, i],
            recv_sem=z_recv.at[way, d, i],
            device_id=(me + step_to[way], core),
            device_id_type=MESH,
        )

    def arrive(way, d, i):
        first, last, _ = cuts[i]
        ref = lists[way][d - 1].at[pl.ds(first, last - first)]
        pltpu.make_async_remote_copy(
            src_ref=ref,
            dst_ref=ref,
            send_sem=z_send.at[way, d - 1, i],
            recv_sem=z_recv.at[way, d - 1, i],
            device_id=(me, 1 - core),
            device_id_type=MESH,
        ).wait_recv()

    def near_hop(way):
        return pltpu.make_async_remote_copy(
            src_ref=near_own,
            dst_ref=near[way],
            send_sem=near_send.at[0],
            recv_sem=near_recv.at[way],
            device_id=(me + step_to[way], core),
            device_id_type=MESH,
        )

    def near_arrive(way):
        pltpu.make_async_remote_copy(
            src_ref=near[way],
            dst_ref=near[way],
            send_sem=near_send.at[0],
            recv_sem=near_recv.at[way],
            device_id=(me, 1 - core),
            device_id_type=MESH,
        ).wait_recv()

    def forward(d, i, here):
        need = cuts[i][2]
        if need > reach - d:
            return
        for way in range(2):

            def go(way=way):
                arrive(way, d, i)
                hop(way, d, i).start()

            pl.when(here(way) & (behind[way] >= d) & (beyond[way] >= need))(go)

    def keep(d, here):
        for i, (_, _, need) in enumerate(cuts):
            if need > reach - d + 1:
                continue
            for way in range(2):
                pl.when(here(way) & (behind[way] >= d) & (beyond[way] + 1 == need))(lambda way=way, i=i: arrive(way, d, i))


    def spread_copy(rel, q):
        mate = z * side + mate_of(rel)
        return pltpu.make_async_remote_copy(
            src_ref=picked.at[rel - 1, pl.ds(q * most, most)],
            dst_ref=final.at[pl.ds((c * planes + q) * most, most)],
            send_sem=in_send.at[rel - 1, q],
            recv_sem=in_recv.at[c * planes + q],
            device_id=(mate, core),
            device_id_type=MESH,
        )

    mates = list(range(side - 1, 0, -1))

    def pick(src, q, k):
        for j in range(most):
            slot = src[tab[8 + q * most + j, mate_of(k) if k else c]]
            if k:
                picked[k - 1, q * most + j] = slot
            else:
                final[(c * planes + q) * most + j] = slot

    def spread(src, q):
        for n, k in enumerate((*mates, 0)):
            pick(src, q, k)
            if n:
                spread_copy(mates[n - 1], q).start()

    def spread_from(d, here):
        for way in range(2):
            q = z - d if way == 0 else z + d
            pl.when(here(way) & (behind[way] >= d))(lambda way=way, q=q: spread(lists[way][d - 1], q))

    def spread_near():
        for way in range(2):

            def go(way=way):
                near_arrive(way)
                spread(near[way], z - 1 if way == 0 else z + 1)

            pl.when((behind[way] == 1) & (beyond[way] >= 1))(go)

    with jax.named_scope("build"):
        for way in range(2):
            for s in range(caps[-1]):
                own_lists[way, s] = kv[tab[way, s]]
        for s in range(caps[0]):
            near_own[s] = kv[tab[4, s]]
        for k in range(side):
            pick(kv, z, k)
    with jax.named_scope("greet"):
        pl.semaphore_wait(barrier, side + (z + reach - 1) // reach + (beyond[0] + reach - 1) // reach)
    with jax.named_scope("first_sends"):
        for way in range(2):
            pl.when(behind[way] == 0)(lambda way=way: near_hop(way).start())
        for i, (_, _, need) in enumerate(cuts):
            for way in range(2):
                pl.when(beyond[way] >= need)(lambda way=way, i=i: hop(way, 0, i).start())
        for k in mates:
            spread_copy(k, z).start()
        for copy in weight_swaps:
            copy.start()

    def norm(lo, hi, rows=32):
        def body(i, carry):
            at = pl.ds(pl.multiple_of(i * rows, rows), rows)
            normed[at, :] = rms_rows(normed[at, :].astype(F32), gain_ref[...]).astype(BF16)
            return carry

        lax.fori_loop(lo // rows, hi // rows, body, 0)

    piece = math.gcd(tokens, 256)
    pieces = tokens // piece
    halo = pool_in.shape[0] - tokens
    groups, group_dim = mix_ref.shape[:2]

    def project_rows(lo, hi):
        def body(i, carry):
            at = pl.ds(pl.multiple_of(i * piece, piece), piece)
            rows = normed[at, :]
            pool_in[pl.ds(pl.multiple_of(halo + i * piece, halo), piece), :] = jnp.dot(
                rows, w_pool[...], preferred_element_type=F32
            ).astype(BF16)
            query[at, :] = jnp.dot(rows, w_query[...], preferred_element_type=F32).astype(BF16)
            return carry

        lax.fori_loop(lo, hi, body, 0)

    def pool_rows(i, carry):
        at = pl.ds(pl.multiple_of(i * piece, piece), piece)
        position = i * piece + lax.broadcasted_iota(jnp.int32, (piece, 1), 0)
        for g in range(groups):
            cols = slice(g * group_dim, (g + 1) * group_dim)
            wide = pool_in[pl.ds(pl.multiple_of(i * piece, piece), piece + halo), cols].astype(F32)
            sums = []
            total = wide
            shift = 1
            while shift < halo:
                total = total + pltpu.roll(total, shift, 0)
                sums.append(total[halo:])
                shift *= 2
            per_core = [sums[k * groups + g] for k in range(len(sums) // groups)]
            level = per_core[0]
            window = 2 ** (g + 1)
            for k in range(1, len(per_core)):
                level = jnp.where(core == k, per_core[k], level)
                window = jnp.where(core == k, 2 ** (k * groups + g + 1), window)
            count = jnp.minimum(position + 1, window).astype(F32)
            pooled = (level / count - wide[halo:]).astype(BF16)
            pool_out[at, cols] = jnp.dot(pooled, mix_ref[g], preferred_element_type=F32).astype(BF16)
        return carry

    def gate_rows(lo, hi):
        def body(i, carry):
            at = pl.ds(pl.multiple_of(i * piece, piece), piece)
            for j in range(2):
                cols = slice(j * half // 2, (j + 1) * half // 2)
                logits = jnp.dot(normed[at, :], w_gate[:, cols], preferred_element_type=F32)
                gate[at, cols] = 1.0 / (1.0 + jnp.exp(-logits))
            return carry

        lax.fori_loop(lo, hi, body, 0)

    def two_terms(a, w, a_far, w_far):
        near = jnp.dot(a, w, preferred_element_type=F32).astype(BF16).astype(F32)
        far = jnp.dot(a_far, w_far, preferred_element_type=F32).astype(BF16).astype(F32)
        return near + far

    def branch_rows(i, carry):
        at = pl.ds(pl.multiple_of(i * piece, piece), piece)
        for j in range(2):
            cols = slice(j * half // 2, (j + 1) * half // 2)
            branch[at, cols] = two_terms(
                pool_out[at, :], w_branch[:, cols], pool_far[at, :], w_branch_far[:, cols]
            )
        return carry

    def at_edge(way):
        return beyond[way] == 0

    def inside(way):
        return beyond[way] >= 1

    def from_edge(way):
        return behind[way] == 1

    def from_inside(way):
        return behind[way] >= 2

    with jax.named_scope("norm"):
        loads[0].wait()
        norm(0, tokens)
    with jax.named_scope("project"):
        loads[1].wait()
        loads[2].wait()
        pool_in[:halo, :] = jnp.zeros((halo, pool_in.shape[1]), BF16)
        project_rows(0, pieces)
    with jax.named_scope("pool"):
        lax.fori_loop(0, pieces, pool_rows, 0)
        pool_swap.start()
    with jax.named_scope("step0"):
        forward(1, 0, from_inside)
    with jax.named_scope("gate"):
        loads[4].wait()
        gate_rows(0, pieces // 2)
    with jax.named_scope("step1"):
        forward(1, 1, from_inside)
        keep(1, at_edge)
        spread_from(1, at_edge)
        spread_near()
    with jax.named_scope("gate"):
        gate_rows(pieces // 2, pieces)
    with jax.named_scope("branch"):
        loads[3].wait()
        loads[5].wait()
        for copy in weight_swaps:
            copy.wait()
        pool_swap.wait()
        lax.fori_loop(0, pieces, branch_rows, 0)
    with jax.named_scope("step2"):
        for i in range(2, len(cuts)):
            forward(1, i, from_inside)
        keep(1, inside)
        spread_from(1, lambda way: inside(way) & from_inside(way))
        forward(1, 0, from_edge)
    for d in range(2, planes):
        with jax.named_scope(f"step{d + 1}"):
            forward(d, 0, inside)
            keep(d, at_edge)
            spread_from(d, at_edge)
            if d == 2:
                for i in range(1, len(cuts)):
                    forward(1, i, from_edge)
            for i in range(1, len(cuts)):
                forward(d, i, inside)
            keep(d, inside)
            spread_from(d, inside)

    with jax.named_scope("arrivals"):
        for rel in range(1, side):
            source = mate_of(rel)
            for q in range(planes):
                at = pl.ds((source * planes + q) * most, most)
                pltpu.make_async_remote_copy(
                    src_ref=final.at[at],
                    dst_ref=final.at[at],
                    send_sem=in_send.at[rel - 1, q],
                    recv_sem=in_recv.at[source * planes + q],
                    device_id=(me, 1 - core),
                    device_id_type=MESH,
                ).wait_recv()

    blocks = tokens // block_len
    heads = scale_ref.shape[0]
    width = query.shape[1]
    head_dim = width // heads
    reads = blocks * per_block
    slot_base = lax.rem(c, 128 // reads) * reads

    def read_swap(b):
        at = pl.ds(pl.multiple_of(b * block_len, block_len), block_len)
        return partner(read.at[at], read_far.at[at], 3 + b)

    def attend_block(b):
        at = pl.ds(pl.multiple_of(b * block_len, block_len), block_len)
        memory = jnp.concatenate(
            [final[tab[2, slot_base + b * per_block + i]] for i in range(per_block)], axis=0
        )
        for h in range(heads):
            cut = slice(h * head_dim, (h + 1) * head_dim)
            scale = scale_ref[h] * (1.0 / math.sqrt(head_dim))
            scores = lax.dot_general(
                query[at, cut], memory[:, cut], (((1,), (1,)), ((), ())), preferred_element_type=F32
            )
            scores = scores * scale
            top = jnp.exp(scores - jnp.max(scores, axis=-1, keepdims=True))
            weights = (top * (1.0 / jnp.sum(top, axis=-1, keepdims=True))).astype(BF16)
            read[at, cut] = jnp.dot(
                weights, memory[:, width + h * head_dim : width + (h + 1) * head_dim], preferred_element_type=F32
            ).astype(BF16)

    unroll = math.gcd(blocks, 4)

    def attend(i, carry):
        for k in range(unroll):
            attend_block(i * unroll + k)
        for k in range(unroll):
            read_swap(i * unroll + k).start()
        return carry

    with jax.named_scope("attend"):
        lax.fori_loop(0, blocks // unroll, attend, 0)

    joint = math.gcd(blocks, 2)

    def out_copy(i):
        at = pl.ds(pl.multiple_of(i * joint * block_len, block_len), joint * block_len)
        return pltpu.make_async_copy(out_rows.at[at], out_ref.at[at], out_sem.at[i])

    def finish(i, carry):
        at = pl.ds(pl.multiple_of(i * joint * block_len, block_len), joint * block_len)
        for k in range(joint):
            read_swap(i * joint + k).wait()
        for j in range(2):
            cols = slice(j * half // 2, (j + 1) * half // 2)
            terms = two_terms(read[at, :], w_out[:, cols], read_far[at, :], w_out_far[:, cols])
            out_rows[at, cols] = (branch[at, cols] + gate[at, cols] * terms).astype(BF16)
        out_copy(i).start()
        return carry

    with jax.named_scope("finish"):
        lax.fori_loop(0, blocks // joint, finish, 0)

    for way in range(2):
        for i, (_, _, need) in enumerate(cuts):
            for d in range(reach - need + 1):
                pl.when((behind[way] >= d) & (beyond[way] >= need))(
                    lambda way=way, d=d, i=i: hop(way, d, i).wait_send()
                )
    for rel in range(1, side):
        for q in range(planes):
            spread_copy(rel, q).wait_send()
    for way in range(2):
        pl.when(behind[way] == 0)(lambda way=way: near_hop(way).wait_send())
    for i in range(blocks // joint):
        out_copy(i).wait()


def mixer(planes, most, block_len, per_block, caps, collective_id, *operands):
    tab, scale, gain, mix, kv, hidden, w_pool, w_query, w_gate, w_branch, w_out = operands
    holders = lax.axis_size("st")
    side = holders // planes
    reach = planes - 1
    tokens, model = hidden.shape
    half = w_gate.shape[1]
    pool_width, width = w_pool.shape[1], w_query.shape[1]
    slot = kv.shape[1:]
    cores = lax.axis_size("tp")
    halo = 2 ** (cores * mix.shape[0])
    nch = len(chunks_of(caps))
    blocks = tokens // block_len
    v = pltpu.VMEM
    dma = pltpu.SemaphoreType.DMA
    flops = 2 * tokens * (model * (pool_width + width + half) + 2 * (pool_width + width) * half)
    return pl.pallas_call(
        functools.partial(mixer_kernel, planes, caps, most, block_len, per_block),
        out_shape=jax.ShapeDtypeStruct((tokens, half), BF16),
        in_specs=[SMEM, SMEM, VMEM, VMEM, VMEM] + [PIN] * 6,
        out_specs=ANY,
        scratch_shapes=[
            v(hidden.shape, BF16),
            v(w_pool.shape, BF16),
            v(w_query.shape, BF16),
            v(w_gate.shape, BF16),
            v((pool_width, half), BF16),
            v((pool_width, half), BF16),
            v((width, half), BF16),
            v((width, half), BF16),
            v((tokens + halo, pool_width), BF16),
            v((tokens, pool_width), BF16),
            v((tokens, pool_width), BF16),
            v((tokens, half), F32),
            v((tokens, half), F32),
            v((tokens, width), BF16),
            v((tokens, width), BF16),
            v((tokens, width), BF16),
            v((2, caps[-1], *slot), BF16),
            *[v((caps[min(reach - d, reach - 2)], *slot), BF16) for _ in range(2) for d in range(1, planes)],
            *[v((caps[0], *slot), BF16) for _ in range(3)],
            v((side - 1, planes * most, *slot), BF16),
            v((holders * most, *slot), BF16),
            v((tokens, half), BF16),
            dma((6,)),
            dma((blocks,)),
            dma((1,)),
            dma((2,)),
            dma((2, reach, nch)),
            dma((2, reach, nch)),
            dma((side - 1, planes)),
            dma((holders,)),
            dma((3 + blocks,)),
            dma((3 + blocks,)),
        ],
        compiler_params=pltpu.CompilerParams(
            collective_id=collective_id, has_side_effects=True, vmem_limit_bytes=55 * 2**20
        ),
        cost_estimate=pl.CostEstimate(flops=flops, bytes_accessed=32 * 2**20, transcendentals=0),
    )(*operands)


def body(
    planes,
    hidden,
    norm_gain,
    store,
    store_gain,
    passage_ids,
    w_pool,
    pool_mix,
    w_branch,
    w_query,
    w_key,
    w_value,
    sharpness,
    w_out,
    w_gate,
):
    holders = lax.axis_size("st")
    side = holders // planes
    blocks, per_block = passage_ids.shape
    reads = blocks * per_block
    pass_dev = store.shape[0]
    tokens, model = hidden.shape
    most = max(1, 2 * reads // holders)

    one = min(pass_dev, side * most)
    full = tuple(min(pass_dev, k * one) for k in range(1, planes - 1))
    variants = []
    for sixteenths in (9, 10, 11):
        first = one * sixteenths // 16
        lengths = (first, first + pass_dev // 6)
        variants.append(tuple(map(min, lengths, full)))
    variants = (*variants, full)
    tab, own_kv = project(planes, most, variants, passage_ids, store, store_gain, w_key, w_value)
    operands = (
        tab,
        sharpness,
        norm_gain.reshape(1, model),
        pool_mix,
        own_kv,
        hidden,
        w_pool,
        w_query,
        w_gate,
        w_branch,
        w_out,
    )
    run = functools.partial(mixer, planes, most, tokens // blocks, per_block)
    return lax.switch(
        tab[3, 0], [functools.partial(run, caps, i + 1) for i, caps in enumerate(variants)], *operands
    )


def solution(mesh):
    placed = (
        P("st", None),
        P(),
        P("st", None, None),
        P(),
        P("st", None),
        P(None, "tp"),
        P("tp", None, None),
        P("tp", None),
        P(None, "tp"),
        P(None, "tp"),
        P(None, "tp"),
        P("tp"),
        P("tp", None),
        P(None, "tp"),
    )
    return jax.shard_map(
        functools.partial(body, planes_of(mesh)), mesh=mesh, in_specs=placed, out_specs=P("st", "tp"), check_vma=False
    )
```
